32 devices in a mesh: rep: 2 (over x), fs: 8 (over z, y), tp: 2 (over core).
Axes of the slice: x: 2, y: 2, z: 4, core: 2. Of those that a mesh axis runs over, the one named last changes fastest.
Arguments:
- x_early: bfloat16 [1792, 2048], P(('rep', 'fs')), may hold values from -6 to 6
- x_late: bfloat16 [1792, 2048], P(('rep', 'fs')), may hold values from -6 to 6
- grad_out: bfloat16 [1792, 2048], P(('rep', 'fs')), may hold values from -6 to 6
- w_gate: bfloat16 [2048, 3072], P('fs', 'tp'), may hold values from -0.125 to 0.125
- w_up: bfloat16 [2048, 3072], P('fs', 'tp'), may hold values from -0.125 to 0.125
- w_down: bfloat16 [3072, 2048], P('tp', 'fs'), may hold values from -0.109375 to 0.109375
- gate_sum: float32 [2048, 3072], P('fs', 'tp'), may hold values from -80 to 80
- up_sum: float32 [2048, 3072], P('fs', 'tp'), may hold values from -80 to 80
- down_sum: float32 [3072, 2048], P('tp', 'fs'), may hold values from -80 to 80
Outputs:
- out_late: bfloat16 [1792, 2048], P(('rep', 'fs'))
- grad_in: bfloat16 [1792, 2048], P(('rep', 'fs'))
- new_gate_sum: float32 [2048, 3072], P('fs', 'tp')
- new_up_sum: float32 [2048, 3072], P('fs', 'tp')
- new_down_sum: float32 [3072, 2048], P('tp', 'fs')
The draws below stay inside these ranges and needn't reach their ends.
All inputs are finite; a program needn't handle non-finite values.
Results may differ from the reference program's by a relative error of at most 0.018.
Values may be sent and summed in bfloat16 or wider, within the bound.
A program may use at most 128 MiB of HBM per device.

```python
import jax
import jax.numpy as jnp
from jax import lax

D = 2048
FF = 3072
TOKENS = 1792
N_TP = 2


def strengthened(drawn, key, source, target, blocks, factor):
    def block_of(dim):
        return (jnp.arange(drawn.shape[dim]) // (drawn.shape[dim] // blocks)).reshape((-1,) + (1,) * (drawn.ndim - 1 - dim))

    one_side = jax.random.permutation(key, blocks)[block_of(target)]
    second = (block_of(target) + blocks // 2) % blocks
    return jnp.where((block_of(source) == one_side) | (block_of(source) == second), factor * drawn, drawn)


def steps_of(rng, extent, split, low, high):
    level, own = 1.0, jax.random.fold_in(rng, 6)
    for position, shards_of in split:
        heights = jnp.exp(jax.random.uniform(jax.random.fold_in(own, position), (shards_of,), jnp.float32, low / len(split), high / len(split)))
        level = level * jnp.repeat(heights, extent[position] // shards_of).reshape([-1 if axis == position else 1 for axis in range(len(extent))])
    return level


def bell_draw(key, extent, scale, most, cuts=(), kind=jnp.bfloat16):
    drawn = jax.random.normal(key, extent, jnp.float32) * scale
    if len(cuts) > 0:
        drawn = steps_of(key, extent, cuts, -0.22, 0.18) * drawn
    return jnp.clip(drawn, min=-most, max=most).astype(kind)


def bell_draw_with(rng, dims, spread, limit, split, heavy, dtype=jnp.bfloat16):
    array = spread * jax.random.normal(rng, dims, jnp.float32)
    if split:
        array = array * steps_of(rng, dims, split, -0.22, 0.18)
    return jnp.clip(strengthened(array, jax.random.fold_in(rng, 3), *heavy), -limit, limit).astype(dtype)


def setup_inputs(seed: int = 0) -> dict:
    seeds = jax.random.split(jax.random.key(seed), 10)
    return {
        "x_early": bell_draw(seeds[0], (TOKENS, D), 1.0, 6.0, ((0, 16),)),
        "x_late": bell_draw(seeds[1], (TOKENS, D), 1.0, 6.0, ((0, 16),)),
        "grad_out": bell_draw_with(seeds[2], (TOKENS, D), 1.0, 6.0, ((0, 16),), (0, 1, 16, 2.0)),
        "w_gate": bell_draw(seeds[3], (D, FF), D ** -0.5, 0.125, ((0, 8), (1, 2))),
        "w_up": bell_draw(seeds[4], (D, FF), D ** -0.5, 0.125, ((0, 8), (1, 2))),
        "w_down": bell_draw(seeds[5], (FF, D), FF ** -0.5, 0.109375, ((0, 2), (1, 8))),
        "gate_sum": bell_draw(seeds[6], (D, FF), (0.3 * TOKENS ** 0.5), 80.0, ((0, 8), (1, 2)), jnp.float32),
        "up_sum": bell_draw(seeds[7], (D, FF), (0.3 * TOKENS ** 0.5), 80.0, ((0, 8), (1, 2)), jnp.float32),
        "down_sum": bell_draw(seeds[8], (FF, D), (0.3 * TOKENS ** 0.5), 80.0, ((0, 2), (1, 8)), jnp.float32),
    }


epsilon = 1e-06

def prepare(x_rows):
    wide = x_rows.astype(jnp.float32)
    row_scale = lax.rsqrt(lax.optimization_barrier(jnp.mean(wide * wide, axis=-1, keepdims=True)) + epsilon)
    normed = (wide * row_scale).astype(jnp.bfloat16)
    return (wide, row_scale, normed)

def reference(x_early, x_late, grad_out, w_gate, w_up, w_down, gate_sum, up_sum, down_sum):
    late_wide, late_scale, late_normed = prepare(x_late)
    late_gate = jnp.dot(late_normed, w_gate, preferred_element_type=jnp.float32)
    late_upper = jnp.dot(late_normed, w_up, preferred_element_type=jnp.float32)
    late_hidden = (late_gate * jax.nn.sigmoid(late_gate) * late_upper).astype(jnp.bfloat16)
    block = FF // N_TP
    branch = jnp.zeros(x_late.shape, jnp.float32)
    for column in range(N_TP):
        part = jnp.dot(late_hidden[:, column * block:(column + 1) * block], w_down[column * block:(column + 1) * block], preferred_element_type=jnp.float32)
        branch = branch + part.astype(jnp.bfloat16).astype(jnp.float32)
    out_late = (late_wide + 0.5 * branch).astype(jnp.bfloat16)
    early_wide, early_scale, early_normed = prepare(x_early)
    gate_pre = jnp.dot(early_normed, w_gate, preferred_element_type=jnp.float32)
    up_pre = jnp.dot(early_normed, w_up, preferred_element_type=jnp.float32)
    gate_sig = jax.nn.sigmoid(gate_pre)
    hidden = (gate_pre * gate_sig * up_pre).astype(jnp.bfloat16)
    grad_hidden = 0.5 * jnp.dot(grad_out, w_down.T, preferred_element_type=jnp.float32)
    grad_gate_in = (grad_hidden * up_pre * gate_sig * (1.0 + gate_pre * (1.0 - gate_sig))).astype(jnp.bfloat16)
    grad_up_in = (grad_hidden * gate_pre * gate_sig).astype(jnp.bfloat16)
    grad_normed = jnp.dot(grad_gate_in, w_gate.T, preferred_element_type=jnp.float32)
    grad_normed = grad_normed + jnp.dot(grad_up_in, w_up.T, preferred_element_type=jnp.float32)
    unit_rows = early_wide * early_scale
    inner = lax.optimization_barrier(jnp.mean(grad_normed * unit_rows, axis=-1, keepdims=True))
    grad_in = (grad_out.astype(jnp.float32) + early_scale * (grad_normed - unit_rows * inner)).astype(jnp.bfloat16)
    new_gate_sum = gate_sum + jnp.dot(early_normed.T, grad_gate_in, preferred_element_type=jnp.float32)
    new_up_sum = up_sum + jnp.dot(early_normed.T, grad_up_in, preferred_element_type=jnp.float32)
    new_down_sum = down_sum + 0.5 * jnp.dot(hidden.T, grad_out, preferred_element_type=jnp.float32)
    return (out_late, grad_in, new_gate_sum, new_up_sum, new_down_sum)
```

```python
import functools

import jax
import jax.numpy as jnp
from jax import lax
from jax.experimental import pallas as pl
from jax.experimental.pallas import tpu as pltpu
from jax.sharding import PartitionSpec as P

epsilon = 1e-06
MESH = pl.DeviceIdType.MESH
ANY = pl.BlockSpec(memory_space=pl.ANY)
LANES, ROWS = 128, 16


def contract_rows(left, right):
    return lax.dot_general(
        left, right, (((0,), (0,)), ((), ())), preferred_element_type=jnp.float32
    )


def contract_cols(left, right):
    return lax.dot_general(
        left, right, (((1,), (1,)), ((), ())), preferred_element_type=jnp.float32
    )


def greet(peers):
    barrier = pltpu.get_barrier_semaphore()
    for peer in peers:
        pl.semaphore_signal(barrier, inc=1, device_id=peer, device_id_type=MESH)
    pl.semaphore_wait(barrier, len(peers))


def push(src, dst, send_sem, recv_sem, peer):
    copy = pltpu.make_async_remote_copy(
        src_ref=src,
        dst_ref=dst,
        send_sem=send_sem,
        recv_sem=recv_sem,
        device_id=peer,
        device_id_type=MESH,
    )
    return copy


def block(index, size, unit):
    return pl.ds(pl.multiple_of(index * size, unit), size)


def call(body, outs, sems, collective, *args, scratch=()):
    return pl.pallas_call(
        body,
        out_shape=outs,
        in_specs=[ANY] * len(args),
        out_specs=jax.tree.map(lambda _: ANY, outs),
        scratch_shapes=[pltpu.SemaphoreType.DMA((n,)) for n in sems] + list(scratch),
        compiler_params=pltpu.CompilerParams(collective_id=collective, has_side_effects=True),
    )(*args)


def here():
    rep, fs, tp = lax.axis_index("rep"), lax.axis_index("fs"), lax.axis_index("tp")
    return rep, fs, tp, {"rep": 1 - rep}, {"tp": 1 - tp}


def gather_kernel(n, acts, weights, acts_all, weights_all, send, recv, wsend, wrecv):
    rep, fs, tp, twin, mate = here()
    line = n // 2
    z, y = fs // 2, lax.rem(fs, 2)
    side = {"fs": fs + 1 - 2 * y}
    rows, width = acts.shape[1], acts.shape[2]
    half = width // 2
    piece = weights_all.shape[1]
    part = piece // 2
    depth = weights.shape[2]
    mine = block(tp, half, LANES)
    greet([twin, mate] + [{"fs": lax.rem(fs + k, n)} for k in range(1, n)])

    def spot(origin):
        return acts_all.at[:, block(origin, rows, ROWS), mine]

    def other_spot(origin):
        return acts_all.at[:, block(origin, rows, ROWS), block(1 - tp, half, LANES)]

    right0, left0, side0, mate0 = 1, 1 + line, 1 + 2 * line, 1 + 3 * line
    own = acts.at[:, :, mine]
    up, down = {"fs": lax.rem(fs + 2, n)}, {"fs": lax.rem(fs + n - 2, n)}

    def go_up(s):
        src = own if s == 0 else spot(fs - 2 * s)
        return push(src, spot(fs - 2 * s), send.at[right0 + s], recv.at[right0 + s], up)

    def go_down(s):
        src = own if s == 0 else spot(fs + 2 * s)
        return push(src, spot(fs + 2 * s), send.at[left0 + s], recv.at[left0 + s], down)

    def go_side(s, sign):
        origin = fs + 2 * sign * s
        src = own if s == 0 else spot(origin)
        at = side0 + origin // 2
        return push(src, spot(origin), send.at[at], recv.at[at], side)

    def go_mate(origin):
        at = mate0 + origin
        return push(spot(origin), spot(origin), send.at[at], recv.at[at], mate)

    def weight(k):
        to = lax.rem(fs + k, n)
        src = weights.at[:, block(to * 2 + rep, part, ROWS), :]
        dst = weights_all.at[:, block(rep, part, ROWS), block(fs, depth, LANES)]
        return push(src, dst, wsend.at[k], wrecv.at[k], {"fs": to})

    def weight_on(k):
        origin = lax.rem(fs + n - k, n)
        ref = weights_all.at[:, block(rep, part, ROWS), block(origin, depth, LANES)]
        return push(ref, ref, wsend.at[n + k], wrecv.at[n + k], twin)

    def weight_from_twin(k):
        origin = lax.rem(fs + n - k, n)
        ref = weights_all.at[:, block(1 - rep, part, ROWS), block(origin, depth, LANES)]
        return push(ref, ref, wsend.at[n + k], wrecv.at[n + k], twin)

    own_weight = push(
        weights.at[:, block(fs, piece, ROWS), :],
        weights_all.at[:, :, block(fs, depth, LANES)],
        wsend.at[0],
        wrecv.at[0],
        twin,
    )
    own_mate = push(acts, acts_all.at[:, block(fs, rows, ROWS), :], send.at[0], recv.at[0], mate)

    has_up = lambda s: (z - s >= 0) & (z + 1 < line)
    has_down = lambda s: (z + s < line) & (z - 1 >= 0)
    from_below = lambda s: z - 1 - s >= 0
    from_above = lambda s: z + 1 + s < line

    pl.when(has_up(0))(lambda: go_up(0).start())
    pl.when(has_down(0))(lambda: go_down(0).start())
    go_side(0, 1).start()
    own_mate.start()
    own_weight.start()
    order = sorted(range(1, n), key=lambda k: -min(k, n - k))
    groups = [order[g :: line] for g in range(line)]

    for s in range(line - 1):
        for k in groups[s]:
            weight(k).start()

        def below():
            push(spot(fs - 2 * (s + 1)), spot(fs - 2 * (s + 1)), send.at[right0 + s], recv.at[right0 + s], up).wait_recv()
            if s + 1 < line - 1:
                pl.when(has_up(s + 1))(lambda: go_up(s + 1).start())
            go_side(s + 1, -1).start()
            go_mate(fs - 2 * (s + 1)).start()

        def above():
            push(spot(fs + 2 * (s + 1)), spot(fs + 2 * (s + 1)), send.at[left0 + s], recv.at[left0 + s], up).wait_recv()
            if s + 1 < line - 1:
                pl.when(has_down(s + 1))(lambda: go_down(s + 1).start())
            go_side(s + 1, 1).start()
            go_mate(fs + 2 * (s + 1)).start()

        pl.when(from_below(s))(below)
        pl.when(from_above(s))(above)
    for k in groups[line - 1]:
        weight(k).start()

    def side_in(place):
        origin = place * 2 + (1 - y)
        at = side0 + place
        push(spot(origin), spot(origin), send.at[at], recv.at[at], side).wait_recv()
        go_mate(origin).start()

    side_in(z)
    for k in order:
        origin = lax.rem(fs + n - k, n)
        ref = weights_all.at[:, block(rep, part, ROWS), block(origin, depth, LANES)]
        push(ref, ref, wsend.at[k], wrecv.at[k], twin).wait_recv()
        weight_on(k).start()
    for s in range(1, line):
        pl.when(z - s >= 0)(lambda: side_in(z - s))
        pl.when(z + s < line)(lambda: side_in(z + s))

    own_mate.wait()
    own_weight.wait()
    for k in range(1, n):
        weight_from_twin(k).wait_recv()
        weight_on(k).wait_send()
        weight(k).wait_send()
        origin = lax.rem(fs + k, n)
        at = mate0 + origin
        ref = other_spot(origin)
        push(ref, ref, send.at[at], recv.at[at], mate).wait()
    for s in range(line - 1):
        pl.when(has_up(s))(lambda: go_up(s).wait_send())
        pl.when(has_down(s))(lambda: go_down(s).wait_send())
    for place in range(line):
        ref = spot(place * 2 + y)
        push(ref, ref, send.at[side0 + place], recv.at[side0 + place], side).wait_send()


def halves_kernel(parts, grads, parts_in, grads_in, send, recv):
    rep, fs, tp, twin, mate = here()
    half = parts.shape[2] // 2
    part = grads.shape[1] // 2
    greet([twin, mate])
    one = push(
        parts.at[:, :, block(1 - tp, half, LANES)], parts_in, send.at[0], recv.at[0], mate
    )
    two = push(grads.at[:, block(1 - rep, part, ROWS), :], grads_in, send.at[1], recv.at[1], twin)
    one.start()
    two.start()
    one.wait()
    two.wait()


def pair_kernel(n, parts, grads, parts_in, grads_all, send, recv, stage, local):
    rep, fs, tp, twin, mate = here()
    y = lax.rem(fs, 2)
    side = {"fs": fs + 1 - 2 * y}
    part = grads.shape[1]
    depth = grads_all.shape[2]
    greet([twin] + [{"fs": lax.rem(fs + k, n)} for k in range(1, n)])
    across = push(parts.at[:, :, 1 - y], parts_in, send.at[0], recv.at[0], side)

    def slot(origin, who):
        return grads_all.at[:, block(origin * 2 + who, part, ROWS), :]

    def share(k):
        to = lax.rem(fs + k, n)
        src = grads.at[:, :, block(to, depth, LANES)]
        return push(src, slot(fs, rep), send.at[k], recv.at[k], {"fs": to})

    def share_on(k):
        origin = lax.rem(fs + n - k, n)
        return push(slot(origin, rep), slot(origin, rep), send.at[n + k], recv.at[n + k], twin)

    def share_from_twin(k):
        origin = lax.rem(fs + n - k, n)
        ref = slot(origin, 1 - rep)
        return push(ref, ref, send.at[n + k], recv.at[n + k], twin)

    order = sorted(range(1, n), key=lambda k: -min(k, n - k))
    for k in order:
        share(k).start()
    across.start()
    own = grads.at[:, :, block(fs, depth, LANES)]
    own_twin = push(own, slot(fs, rep), send.at[n], recv.at[n], twin)
    own_twin.start()
    take = pltpu.make_async_copy(own, stage, local.at[0])
    take.start()
    take.wait()
    put = pltpu.make_async_copy(stage, slot(fs, rep), local.at[1])
    put.start()
    for k in order:
        origin = lax.rem(fs + n - k, n)
        ref = slot(origin, rep)
        push(ref, ref, send.at[k], recv.at[k], twin).wait_recv()
        share_on(k).start()
    put.wait()
    across.wait()
    own_twin.wait_send()
    ref = slot(fs, 1 - rep)
    push(ref, ref, send.at[n], recv.at[n], twin).wait_recv()
    for k in order:
        share(k).wait_send()
        share_on(k).wait_send()
        share_from_twin(k).wait_recv()


def line_kernel(n, parts, parts_in, send, recv):
    rep, fs, tp, twin, mate = here()
    line = n // 2
    z = fs // 2
    greet([{"fs": lax.rem(fs + 2 * k, n)} for k in range(1, line)])

    def copy(k):
        to = lax.rem(z + k, line)
        return push(
            parts.at[:, to],
            parts_in.at[k - 1],
            send.at[k],
            recv.at[k],
            {"fs": lax.rem(fs + 2 * k, n)},
        )

    for k in range(1, line):
        copy(k).start()
    for k in range(1, line):
        copy(k).wait()


def mate_kernel(sums, sums_in, send, recv):
    rep, fs, tp, twin, mate = here()
    greet([mate])
    copy = push(sums, sums_in, send.at[0], recv.at[0], mate)
    copy.start()
    copy.wait()


def fast_shards(n, x_early, x_late, grad_out, w_gate, w_up, w_down, gate_sum, up_sum, down_sum):
    bf16, f32 = jnp.bfloat16, jnp.float32
    shape = jax.ShapeDtypeStruct
    rep, fs, tp = lax.axis_index("rep"), lax.axis_index("fs"), lax.axis_index("tp")
    line = n // 2
    y = lax.rem(fs, 2)
    rows, width = x_early.shape
    hidden_here, depth = w_down.shape
    piece = hidden_here // n
    half = width // 2
    early = x_early.astype(f32)
    late = x_late.astype(f32)
    scale_of = lambda v: lax.rsqrt(jnp.mean(v * v, axis=-1, keepdims=True) + epsilon)
    early_scale, late_scale = scale_of(early), scale_of(late)
    acts = jnp.stack(
        [(early * early_scale).astype(bf16), (late * late_scale).astype(bf16), grad_out]
    )
    weights = jnp.stack([w_gate.T, w_up.T, w_down])
    acts_all, weights_all = call(
        functools.partial(gather_kernel, n),
        [shape((3, n * rows, width), bf16), shape((3, piece, width), bf16)],
        (1 + 3 * line + n, 1 + 3 * line + n, 2 * n, 2 * n),
        0,
        acts,
        weights,
    )
    gate_t, up_t, down_t = weights_all[0], weights_all[1], weights_all[2]
    normed, cotangent = acts_all[0], acts_all[2]
    gate_up = weights_all[:2].reshape(2 * piece, width)
    pre = contract_cols(acts_all[:2].reshape(2 * n * rows, width), gate_up)
    gate_pre, up_pre = pre[:, :piece], pre[:, piece:]
    sig = jax.nn.sigmoid(gate_pre)
    hidden = (gate_pre * sig * up_pre).astype(bf16)
    tokens = n * rows
    late_part = jnp.dot(hidden[tokens:], down_t, preferred_element_type=f32).astype(bf16)
    g, u, s = gate_pre[:tokens], up_pre[:tokens], sig[:tokens]
    grad_hidden = 0.5 * contract_cols(cotangent, down_t)
    grad_gate_in = (grad_hidden * u * s * (1.0 + g * (1.0 - s))).astype(bf16)
    grad_up_in = (grad_hidden * g * s).astype(bf16)
    grads_in = jnp.concatenate([grad_gate_in, grad_up_in], axis=1)
    normed_part = jnp.dot(grads_in, gate_up, preferred_element_type=f32).astype(bf16)
    gate_up_delta = contract_rows(grads_in, normed).astype(bf16)
    down_delta = (0.5 * contract_rows(hidden[:tokens], cotangent)).astype(bf16)
    grads = jnp.concatenate([gate_up_delta, down_delta], axis=0).reshape(3, piece, width)
    parts = jnp.stack([late_part, normed_part])
    parts_in, grads_in = call(
        halves_kernel,
        [shape((2, tokens, half), bf16), shape((3, piece // 2, width), bf16)],
        (2, 2),
        1,
        parts,
        grads,
    )
    add = lambda a, b: (a.astype(f32) + b.astype(f32)).astype(bf16)
    parts = add(lax.dynamic_slice_in_dim(parts, tp * half, half, 2), parts_in)
    grads = add(lax.dynamic_slice_in_dim(grads, rep * (piece // 2), piece // 2, 1), grads_in)
    parts = parts.reshape(2, line, 2, rows, half)
    parts_in, grads_all = call(
        functools.partial(pair_kernel, n),
        [shape((2, line, rows, half), bf16), shape((3, hidden_here, depth), bf16)],
        (2 * n, 2 * n),
        2,
        parts,
        grads,
        scratch=(
            pltpu.VMEM((3, piece // 2, depth), bf16),
            pltpu.SemaphoreType.DMA((2,)),
        ),
    )
    parts = add(lax.dynamic_index_in_dim(parts, y, 2, keepdims=False), parts_in)
    parts_in = call(
        functools.partial(line_kernel, n),
        shape((line - 1, 2, rows, half), bf16),
        (line, line),
        3,
        parts,
    )
    sums = lax.dynamic_index_in_dim(parts, fs // 2, 1, keepdims=False).astype(f32)
    sums = (sums + jnp.sum(parts_in.astype(f32), axis=0)).astype(bf16)
    sums_in = call(mate_kernel, shape((2, rows, half), bf16), (1, 1), 4, sums)
    left, right = jnp.where(tp == 0, sums, sums_in), jnp.where(tp == 0, sums_in, sums)
    full = jnp.concatenate([left, right], axis=2).astype(f32)
    branch, grad_normed = full[0], full[1]
    out_late = (late + 0.5 * branch).astype(bf16)
    unit_rows = early * early_scale
    inner = jnp.mean(grad_normed * unit_rows, axis=-1, keepdims=True)
    grad_in = (
        grad_out.astype(f32) + early_scale * (grad_normed - unit_rows * inner)
    ).astype(bf16)
    return (
        out_late,
        grad_in,
        gate_sum + grads_all[0].T.astype(f32),
        up_sum + grads_all[1].T.astype(f32),
        down_sum + grads_all[2].astype(f32),
    )


def shards(x_early, x_late, grad_out, w_gate, w_up, w_down, gate_sum, up_sum, down_sum):
    gate_full, up_full, down_full = (
        lax.all_gather(w_gate, "fs", axis=0, tiled=True),
        lax.all_gather(w_up, "fs", axis=0, tiled=True),
        lax.all_gather(w_down, "fs", axis=1, tiled=True),
    )
    batch_rows = x_early.shape[0]
    stacked = jnp.concatenate([x_early, x_late], axis=0).astype(jnp.float32)
    row_scale = lax.rsqrt(jnp.mean(stacked * stacked, axis=-1, keepdims=True) + epsilon)
    normed = (stacked * row_scale).astype(jnp.bfloat16)
    gate_pre = jnp.dot(normed, gate_full, preferred_element_type=jnp.float32)
    up_pre = jnp.dot(normed, up_full, preferred_element_type=jnp.float32)
    gate_sig = jax.nn.sigmoid(gate_pre)
    hidden = (gate_pre * gate_sig * up_pre).astype(jnp.bfloat16)
    late_part = jnp.dot(hidden[batch_rows:], down_full, preferred_element_type=jnp.float32).astype(
        jnp.bfloat16
    )
    branch = lax.psum(late_part, "tp").astype(jnp.float32)
    out_late = (stacked[batch_rows:] + 0.5 * branch).astype(jnp.bfloat16)
    early_gate = gate_pre[:batch_rows]
    early_upper = up_pre[:batch_rows]
    early_sig = gate_sig[:batch_rows]
    early_hidden = hidden[:batch_rows]
    early_normed = normed[:batch_rows]
    early_scale = row_scale[:batch_rows]
    grad_hidden = 0.5 * contract_cols(grad_out, down_full)
    grad_gate_in = (
        grad_hidden * early_upper * early_sig * (1.0 + early_gate * (1.0 - early_sig))
    ).astype(jnp.bfloat16)
    grad_up_in = (grad_hidden * early_gate * early_sig).astype(jnp.bfloat16)
    normed_part = contract_cols(grad_gate_in, gate_full) + contract_cols(grad_up_in, up_full)
    grad_normed = lax.psum(normed_part.astype(jnp.bfloat16), "tp").astype(jnp.float32)
    unit_rows = stacked[:batch_rows] * early_scale
    inner = jnp.mean(grad_normed * unit_rows, axis=-1, keepdims=True)
    grad_in = (
        grad_out.astype(jnp.float32) + early_scale * (grad_normed - unit_rows * inner)
    ).astype(jnp.bfloat16)
    normed_cols, out_cols = (
        lax.all_to_all(early_normed, "fs", split_axis=1, concat_axis=0, tiled=True),
        lax.all_to_all(grad_out, "fs", split_axis=1, concat_axis=0, tiled=True),
    )
    gate_delta = contract_rows(normed_cols, lax.all_gather(grad_gate_in, "fs", axis=0, tiled=True))
    up_delta = contract_rows(normed_cols, lax.all_gather(grad_up_in, "fs", axis=0, tiled=True))
    down_half = contract_rows(lax.all_gather(early_hidden, "fs", axis=0, tiled=True), out_cols)
    down_delta = 0.5 * down_half
    gate_delta, up_delta, down_delta = (
        lax.psum(gate_delta.astype(jnp.bfloat16), "rep").astype(jnp.float32),
        lax.psum(up_delta.astype(jnp.bfloat16), "rep").astype(jnp.float32),
        lax.psum(down_delta.astype(jnp.bfloat16), "rep").astype(jnp.float32),
    )
    return (out_late, grad_in, gate_sum + gate_delta, up_sum + up_delta, down_sum + down_delta)


def shards_for(mesh):
    n, reps, cores = mesh.shape["fs"], mesh.shape["rep"], mesh.shape["tp"]

    def run(*args):
        rows, width = args[0].shape
        hidden_here, depth = args[5].shape
        fits = (
            reps == 2
            and cores == 2
            and n % 2 == 0
            and rows % ROWS == 0
            and width % (2 * LANES) == 0
            and depth % LANES == 0
            and hidden_here % (2 * n * ROWS) == 0
        )
        return fast_shards(n, *args) if fits else shards(*args)

    return run


def solution(mesh):
    placed = (
        P(("rep", "fs"), None),
        P(("rep", "fs"), None),
        P(("rep", "fs"), None),
        P("fs", "tp"),
        P("fs", "tp"),
        P("tp", "fs"),
        P("fs", "tp"),
        P("fs", "tp"),
        P("tp", "fs"),
    )
    return jax.shard_map(
        shards_for(mesh),
        mesh=mesh,
        in_specs=placed,
        out_specs=(
            P(("rep", "fs"), None),
            P(("rep", "fs"), None),
            P("fs", "tp"),
            P("fs", "tp"),
            P("tp", "fs"),
        ),
        check_vma=False,
    )
```

```python
import functools

import jax
import jax.numpy as jnp
from jax import lax
from jax.experimental import pallas as pl
from jax.experimental.pallas import tpu as pltpu
from jax.sharding import PartitionSpec as P

epsilon = 1e-06
MESH = pl.DeviceIdType.MESH
ANY = pl.BlockSpec(memory_space=pl.ANY)
LANES, ROWS = 128, 16


def contract_rows(left, right):
    return lax.dot_general(
        left, right, (((0,), (0,)), ((), ())), preferred_element_type=jnp.float32
    )


def contract_cols(left, right):
    return lax.dot_general(
        left, right, (((1,), (1,)), ((), ())), preferred_element_type=jnp.float32
    )


def greet(peers):
    barrier = pltpu.get_barrier_semaphore()
    for peer in peers:
        pl.semaphore_signal(barrier, inc=1, device_id=peer, device_id_type=MESH)
    pl.semaphore_wait(barrier, len(peers))


def push(src, dst, send_sem, recv_sem, peer):
    copy = pltpu.make_async_remote_copy(
        src_ref=src,
        dst_ref=dst,
        send_sem=send_sem,
        recv_sem=recv_sem,
        device_id=peer,
        device_id_type=MESH,
    )
    return copy


def block(index, size, unit):
    return pl.ds(pl.multiple_of(index * size, unit), size)


def call(body, outs, sems, collective, *args, scratch=()):
    return pl.pallas_call(
        body,
        out_shape=outs,
        in_specs=[ANY] * len(args),
        out_specs=jax.tree.map(lambda _: ANY, outs),
        scratch_shapes=[pltpu.SemaphoreType.DMA((n,)) for n in sems] + list(scratch),
        compiler_params=pltpu.CompilerParams(collective_id=collective, has_side_effects=True),
    )(*args)


def here():
    rep, fs, tp = lax.axis_index("rep"), lax.axis_index("fs"), lax.axis_index("tp")
    return rep, fs, tp, {"rep": 1 - rep}, {"tp": 1 - tp}


def gather_kernel(n, acts, weights, acts_all, weights_all, send, recv, wsend, wrecv):
    rep, fs, tp, twin, mate = here()
    line = n // 2
    z, y = fs // 2, lax.rem(fs, 2)
    side = {"fs": fs + 1 - 2 * y}
    rows, width = acts.shape[1], acts.shape[2]
    half = width // 2
    piece = weights_all.shape[1]
    part = piece // 2
    depth = weights.shape[2]
    mine = block(tp, half, LANES)
    greet([twin, mate] + [{"fs": lax.rem(fs + k, n)} for k in range(1, n)])

    def spot(origin):
        return acts_all.at[:, block(origin, rows, ROWS), mine]

    def other_spot(origin):
        return acts_all.at[:, block(origin, rows, ROWS), block(1 - tp, half, LANES)]

    right0, left0, side0, mate0 = 1, 1 + line, 1 + 2 * line, 1 + 3 * line
    own = acts.at[:, :, mine]
    up, down = {"fs": lax.rem(fs + 2, n)}, {"fs": lax.rem(fs + n - 2, n)}

    def go_up(s):
        src = own if s == 0 else spot(fs - 2 * s)
        return push(src, spot(fs - 2 * s), send.at[right0 + s], recv.at[right0 + s], up)

    def go_down(s):
        src = own if s == 0 else spot(fs + 2 * s)
        return push(src, spot(fs + 2 * s), send.at[left0 + s], recv.at[left0 + s], down)

    def go_side(s, sign):
        origin = fs + 2 * sign * s
        src = own if s == 0 else spot(origin)
        at = side0 + origin // 2
        return push(src, spot(origin), send.at[at], recv.at[at], side)

    def go_mate(origin):
        at = mate0 + origin
        return push(spot(origin), spot(origin), send.at[at], recv.at[at], mate)

    def weight(k):
        to = lax.rem(fs + k, n)
        src = weights.at[:, block(to * 2 + rep, part, ROWS), :]
        dst = weights_all.at[:, block(rep, part, ROWS), block(fs, depth, LANES)]
        return push(src, dst, wsend.at[k], wrecv.at[k], {"fs": to})

    def weight_on(k):
        origin = lax.rem(fs + n - k, n)
        ref = weights_all.at[:, block(rep, part, ROWS), block(origin, depth, LANES)]
        return push(ref, ref, wsend.at[n + k], wrecv.at[n + k], twin)

    def weight_from_twin(k):
        origin = lax.rem(fs + n - k, n)
        ref = weights_all.at[:, block(1 - rep, part, ROWS), block(origin, depth, LANES)]
        return push(ref, ref, wsend.at[n + k], wrecv.at[n + k], twin)

    own_weight = push(
        weights.at[:, block(fs, piece, ROWS), :],
        weights_all.at[:, :, block(fs, depth, LANES)],
        wsend.at[0],
        wrecv.at[0],
        twin,
    )
    own_mate = push(acts, acts_all.at[:, block(fs, rows, ROWS), :], send.at[0], recv.at[0], mate)

    has_up = lambda s: (z - s >= 0) & (z + 1 < line)
    has_down = lambda s: (z + s < line) & (z - 1 >= 0)
    from_below = lambda s: z - 1 - s >= 0
    from_above = lambda s: z + 1 + s < line

    pl.when(has_up(0))(lambda: go_up(0).start())
    pl.when(has_down(0))(lambda: go_down(0).start())
    go_side(0, 1).start()
    own_mate.start()
    own_weight.start()
    order = sorted(range(1, n), key=lambda k: -min(k, n - k))
    groups = [order[g :: line] for g in range(line)]

    for s in range(line - 1):
        for k in groups[s]:
            weight(k).start()

        def below():
            push(spot(fs - 2 * (s + 1)), spot(fs - 2 * (s + 1)), send.at[right0 + s], recv.at[right0 + s], up).wait_recv()
            if s + 1 < line - 1:
                pl.when(has_up(s + 1))(lambda: go_up(s + 1).start())
            go_side(s + 1, -1).start()
            go_mate(fs - 2 * (s + 1)).start()

        def above():
            push(spot(fs + 2 * (s + 1)), spot(fs + 2 * (s + 1)), send.at[left0 + s], recv.at[left0 + s], up).wait_recv()
            if s + 1 < line - 1:
                pl.when(has_down(s + 1))(lambda: go_down(s + 1).start())
            go_side(s + 1, 1).start()
            go_mate(fs + 2 * (s + 1)).start()

        pl.when(from_below(s))(below)
        pl.when(from_above(s))(above)
    for k in groups[line - 1]:
        weight(k).start()

    def side_in(place):
        origin = place * 2 + (1 - y)
        at = side0 + place
        push(spot(origin), spot(origin), send.at[at], recv.at[at], side).wait_recv()
        go_mate(origin).start()

    side_in(z)
    for k in order:
        origin = lax.rem(fs + n - k, n)
        ref = weights_all.at[:, block(rep, part, ROWS), block(origin, depth, LANES)]
        push(ref, ref, wsend.at[k], wrecv.at[k], twin).wait_recv()
        weight_on(k).start()
    for s in range(1, line):
        pl.when(z - s >= 0)(lambda: side_in(z - s))
        pl.when(z + s < line)(lambda: side_in(z + s))

    own_mate.wait()
    own_weight.wait()
    for k in range(1, n):
        weight_from_twin(k).wait_recv()
        weight_on(k).wait_send()
        weight(k).wait_send()
        origin = lax.rem(fs + k, n)
        at = mate0 + origin
        ref = other_spot(origin)
        push(ref, ref, send.at[at], recv.at[at], mate).wait()
    for s in range(line - 1):
        pl.when(has_up(s))(lambda: go_up(s).wait_send())
        pl.when(has_down(s))(lambda: go_down(s).wait_send())
    for place in range(line):
        ref = spot(place * 2 + y)
        push(ref, ref, send.at[side0 + place], recv.at[side0 + place], side).wait_send()


def add_rows(dst, left, right):
    strip = ROWS
    count = dst.shape[0] // strip

    @pl.loop(0, count)
    def _(i):
        at = pl.ds(pl.multiple_of(i * strip, strip), strip)
        total = left[at, :].astype(jnp.float32) + right[at, :].astype(jnp.float32)
        dst[at, :] = total.astype(dst.dtype)


def reduce_kernel(
    n,
    late,
    norm,
    gate_up,
    down,
    full,
    grads_all,
    p_in,
    p2,
    y_in,
    p3,
    z_in,
    g_in,
    g2,
    sums,
    send,
    recv,
    gsend,
    grecv,
    local,
):
    rep, fs, tp, twin, mate = here()
    line = n // 2
    z, y = fs // 2, lax.rem(fs, 2)
    side = {"fs": fs + 1 - 2 * y}
    half = sums.shape[2]
    rows = sums.shape[1]
    part = g2.shape[1]
    piece = 2 * part
    depth = grads_all.shape[2]
    mine, other = block(tp, half, LANES), block(1 - tp, half, LANES)
    greet([twin, mate] + [{"fs": lax.rem(fs + k, n)} for k in range(1, n)])
    order = sorted(range(1, line), key=lambda k: -min(k, line - k)) + [0]
    far = sorted(range(1, n), key=lambda k: -min(k, n - k))
    side0, line0, x0, last = 2 * line, 3 * line, 4 * line, 4 * line + 3

    def place(k):
        return lax.rem(z + k, line)

    def span(k):
        return block(place(k), 2 * rows, ROWS)

    def to_mate(i, k):
        src = (late, norm)[i].at[span(k), other]
        at = i * line + k
        return push(src, p_in.at[i, span(k), :], send.at[at], recv.at[at], mate)

    def to_side(k):
        src = p2.at[:, block(place(k) * 2 + 1 - y, rows, ROWS), :]
        at = side0 + k
        return push(src, y_in.at[:, place(k)], send.at[at], recv.at[at], side)

    def to_line(k):
        at = line0 + k
        return push(
            p3.at[k], z_in.at[k - 1], send.at[at], recv.at[at], {"fs": lax.rem(fs + 2 * k, n)}
        )

    def delta(a, who):
        if a < 2:
            return gate_up.at[block(2 * a + who, part, ROWS), :]
        return down.at[block(who, part, ROWS), :]

    def to_twin(a):
        return push(delta(a, 1 - rep), g_in.at[a], send.at[x0 + a], recv.at[x0 + a], twin)

    def slot(a, origin, who):
        return grads_all.at[a, block(origin * 2 + who, part, ROWS), :]

    def share(a, k):
        to = lax.rem(fs + k, n)
        src = g2.at[a, :, block(to, depth, LANES)]
        at = a * n + k
        return push(src, slot(a, fs, rep), gsend.at[at], grecv.at[at], {"fs": to})

    def share_in(a, k):
        ref = slot(a, lax.rem(fs + n - k, n), rep)
        at = a * n + k
        return push(ref, ref, gsend.at[at], grecv.at[at], twin)

    def share_on(a, k):
        ref = slot(a, lax.rem(fs + n - k, n), rep)
        at = (3 + a) * n + k
        return push(ref, ref, gsend.at[at], grecv.at[at], twin)

    def share_from_twin(a, k):
        ref = slot(a, lax.rem(fs + n - k, n), 1 - rep)
        at = (3 + a) * n + k
        return push(ref, ref, gsend.at[at], grecv.at[at], twin)

    def own(a):
        return g2.at[a, :, block(fs, depth, LANES)]

    def own_twin(a):
        at = (3 + a) * n
        return push(own(a), slot(a, fs, rep), gsend.at[at], grecv.at[at], twin)

    def own_put(a):
        return pltpu.make_async_copy(own(a), slot(a, fs, rep), local.at[a])

    def weight_step(a):
        to_twin(a).wait_recv()
        add_rows(g2.at[a], delta(a, rep), g_in.at[a])
        for k in far:
            share(a, k).start()
        own_twin(a).start()
        own_put(a).start()

    def forward(a):
        for k in far:
            share_in(a, k).wait_recv()
            share_on(a, k).start()

    for k in order:
        for i in range(2):
            to_mate(i, k).start()
    for a in range(3):
        to_twin(a).start()
    for k in order:
        for i in range(2):
            to_mate(i, k).wait_recv()
            src = (late, norm)[i].at[span(k), mine]
            add_rows(p2.at[i, span(k), :], src, p_in.at[i, span(k), :])
        to_side(k).start()
    weight_step(0)
    for step, k in enumerate(order):
        to_side(k).wait_recv()
        for i in range(2):
            src = p2.at[i, block(place(k) * 2 + y, rows, ROWS), :]
            add_rows(p3.at[k, i], src, y_in.at[i, place(k)])
        if k:
            to_line(k).start()
        if step < 2:
            weight_step(step + 1)
        if step >= 1:
            if step - 1 < 3:
                forward(step - 1)
    for a in range(max(len(order) - 1, 0), 3):
        forward(a)
    for k in order[:-1]:
        to_line(k).wait_recv()
    for i in range(2):

        @pl.loop(0, rows // ROWS)
        def _(j):
            at = pl.ds(pl.multiple_of(j * ROWS, ROWS), ROWS)
            total = p3[0, i, at, :].astype(jnp.float32)
            for k in range(1, line):
                total += z_in[k - 1, i, at, :].astype(jnp.float32)
            sums[i, at, :] = total.astype(sums.dtype)

    out = push(sums, full.at[:, :, mine], send.at[last], recv.at[last], mate)
    out.start()
    keep = pltpu.make_async_copy(sums, full.at[:, :, mine], local.at[3])
    keep.start()
    for a in range(3):
        own_put(a).wait()
        own_twin(a).wait_send()
        ref = slot(a, fs, 1 - rep)
        at = (3 + a) * n
        push(ref, ref, gsend.at[at], grecv.at[at], twin).wait_recv()
        to_twin(a).wait_send()
        for k in far:
            share(a, k).wait_send()
            share_on(a, k).wait_send()
            share_from_twin(a, k).wait_recv()
    for k in order:
        for i in range(2):
            to_mate(i, k).wait_send()
        to_side(k).wait_send()
        if k:
            to_line(k).wait_send()
    keep.wait()
    out.wait_send()
    push(sums, full.at[:, :, other], send.at[last], recv.at[last], mate).wait_recv()


def fast_shards(n, x_early, x_late, grad_out, w_gate, w_up, w_down, gate_sum, up_sum, down_sum):
    bf16, f32 = jnp.bfloat16, jnp.float32
    shape = jax.ShapeDtypeStruct
    rep, fs, tp = lax.axis_index("rep"), lax.axis_index("fs"), lax.axis_index("tp")
    line = n // 2
    y = lax.rem(fs, 2)
    rows, width = x_early.shape
    hidden_here, depth = w_down.shape
    piece = hidden_here // n
    half = width // 2
    early = x_early.astype(f32)
    late = x_late.astype(f32)
    scale_of = lambda v: lax.rsqrt(jnp.mean(v * v, axis=-1, keepdims=True) + epsilon)
    early_scale, late_scale = scale_of(early), scale_of(late)
    acts = jnp.stack(
        [(early * early_scale).astype(bf16), (late * late_scale).astype(bf16), grad_out]
    )
    weights = jnp.stack([w_gate.T, w_up.T, w_down])
    acts_all, weights_all = call(
        functools.partial(gather_kernel, n),
        [shape((3, n * rows, width), bf16), shape((3, piece, width), bf16)],
        (1 + 3 * line + n, 1 + 3 * line + n, 2 * n, 2 * n),
        0,
        acts,
        weights,
    )
    gate_t, up_t, down_t = weights_all[0], weights_all[1], weights_all[2]
    normed, cotangent = acts_all[0], acts_all[2]
    gate_up = weights_all[:2].reshape(2 * piece, width)
    pre = contract_cols(acts_all[:2].reshape(2 * n * rows, width), gate_up)
    gate_pre, up_pre = pre[:, :piece], pre[:, piece:]
    sig = jax.nn.sigmoid(gate_pre)
    hidden = (gate_pre * sig * up_pre).astype(bf16)
    tokens = n * rows
    late_part = jnp.dot(hidden[tokens:], down_t, preferred_element_type=f32).astype(bf16)
    g, u, s = gate_pre[:tokens], up_pre[:tokens], sig[:tokens]
    grad_hidden = 0.5 * contract_cols(cotangent, down_t)
    grad_gate_in = (grad_hidden * u * s * (1.0 + g * (1.0 - s))).astype(bf16)
    grad_up_in = (grad_hidden * g * s).astype(bf16)
    grads_in = jnp.concatenate([grad_gate_in, grad_up_in], axis=1)
    normed_part = jnp.dot(grads_in, gate_up, preferred_element_type=f32).astype(bf16)
    gate_up_delta = contract_rows(grads_in, normed).astype(bf16)
    down_delta = (0.5 * contract_rows(hidden[:tokens], cotangent)).astype(bf16)
    part = piece // 2
    dma = pltpu.SemaphoreType.DMA
    vmem = pl.BlockSpec(memory_space=pltpu.VMEM)
    full, grads_all = pl.pallas_call(
        functools.partial(reduce_kernel, n),
        out_shape=[shape((2, rows, width), bf16), shape((3, hidden_here, depth), bf16)],
        in_specs=[vmem] * 4,
        out_specs=[ANY, ANY],
        scratch_shapes=[
            pltpu.VMEM((2, tokens, half), bf16),
            pltpu.VMEM((2, tokens, half), bf16),
            pltpu.VMEM((2, line, rows, half), bf16),
            pltpu.VMEM((line, 2, rows, half), bf16),
            pltpu.VMEM((line - 1, 2, rows, half), bf16),
            pltpu.VMEM((3, part, width), bf16),
            pltpu.VMEM((3, part, width), bf16),
            pltpu.VMEM((2, rows, half), bf16),
            dma((4 * line + 4,)),
            dma((4 * line + 4,)),
            dma((6 * n,)),
            dma((6 * n,)),
            dma((4,)),
        ],
        compiler_params=pltpu.CompilerParams(
            collective_id=1, has_side_effects=True, vmem_limit_bytes=48 * 2**20
        ),
    )(late_part, normed_part, gate_up_delta, down_delta)
    full = full.astype(f32)
    branch, grad_normed = full[0], full[1]
    out_late = (late + 0.5 * branch).astype(bf16)
    unit_rows = early * early_scale
    inner = jnp.mean(grad_normed * unit_rows, axis=-1, keepdims=True)
    grad_in = (
        grad_out.astype(f32) + early_scale * (grad_normed - unit_rows * inner)
    ).astype(bf16)
    gate_delta, up_delta = lax.optimization_barrier((grads_all[0].T, grads_all[1].T))
    return (
        out_late,
        grad_in,
        gate_sum + gate_delta.astype(f32),
        up_sum + up_delta.astype(f32),
        down_sum + grads_all[2].astype(f32),
    )


def shards(x_early, x_late, grad_out, w_gate, w_up, w_down, gate_sum, up_sum, down_sum):
    gate_full, up_full, down_full = (
        lax.all_gather(w_gate, "fs", axis=0, tiled=True),
        lax.all_gather(w_up, "fs", axis=0, tiled=True),
        lax.all_gather(w_down, "fs", axis=1, tiled=True),
    )
    batch_rows = x_early.shape[0]
    stacked = jnp.concatenate([x_early, x_late], axis=0).astype(jnp.float32)
    row_scale = lax.rsqrt(jnp.mean(stacked * stacked, axis=-1, keepdims=True) + epsilon)
    normed = (stacked * row_scale).astype(jnp.bfloat16)
    gate_pre = jnp.dot(normed, gate_full, preferred_element_type=jnp.float32)
    up_pre = jnp.dot(normed, up_full, preferred_element_type=jnp.float32)
    gate_sig = jax.nn.sigmoid(gate_pre)
    hidden = (gate_pre * gate_sig * up_pre).astype(jnp.bfloat16)
    late_part = jnp.dot(hidden[batch_rows:], down_full, preferred_element_type=jnp.float32).astype(
        jnp.bfloat16
    )
    branch = lax.psum(late_part, "tp").astype(jnp.float32)
    out_late = (stacked[batch_rows:] + 0.5 * branch).astype(jnp.bfloat16)
    early_gate = gate_pre[:batch_rows]
    early_upper = up_pre[:batch_rows]
    early_sig = gate_sig[:batch_rows]
    early_hidden = hidden[:batch_rows]
    early_normed = normed[:batch_rows]
    early_scale = row_scale[:batch_rows]
    grad_hidden = 0.5 * contract_cols(grad_out, down_full)
    grad_gate_in = (
        grad_hidden * early_upper * early_sig * (1.0 + early_gate * (1.0 - early_sig))
    ).astype(jnp.bfloat16)
    grad_up_in = (grad_hidden * early_gate * early_sig).astype(jnp.bfloat16)
    normed_part = contract_cols(grad_gate_in, gate_full) + contract_cols(grad_up_in, up_full)
    grad_normed = lax.psum(normed_part.astype(jnp.bfloat16), "tp").astype(jnp.float32)
    unit_rows = stacked[:batch_rows] * early_scale
    inner = jnp.mean(grad_normed * unit_rows, axis=-1, keepdims=True)
    grad_in = (
        grad_out.astype(jnp.float32) + early_scale * (grad_normed - unit_rows * inner)
    ).astype(jnp.bfloat16)
    normed_cols, out_cols = (
        lax.all_to_all(early_normed, "fs", split_axis=1, concat_axis=0, tiled=True),
        lax.all_to_all(grad_out, "fs", split_axis=1, concat_axis=0, tiled=True),
    )
    gate_delta = contract_rows(normed_cols, lax.all_gather(grad_gate_in, "fs", axis=0, tiled=True))
    up_delta = contract_rows(normed_cols, lax.all_gather(grad_up_in, "fs", axis=0, tiled=True))
    down_half = contract_rows(lax.all_gather(early_hidden, "fs", axis=0, tiled=True), out_cols)
    down_delta = 0.5 * down_half
    gate_delta, up_delta, down_delta = (
        lax.psum(gate_delta.astype(jnp.bfloat16), "rep").astype(jnp.float32),
        lax.psum(up_delta.astype(jnp.bfloat16), "rep").astype(jnp.float32),
        lax.psum(down_delta.astype(jnp.bfloat16), "rep").astype(jnp.float32),
    )
    return (out_late, grad_in, gate_sum + gate_delta, up_sum + up_delta, down_sum + down_delta)


def shards_for(mesh):
    n, reps, cores = mesh.shape["fs"], mesh.shape["rep"], mesh.shape["tp"]

    def run(*args):
        rows, width = args[0].shape
        hidden_here, depth = args[5].shape
        fits = (
            reps == 2
            and cores == 2
            and n % 2 == 0
            and rows % ROWS == 0
            and width % (2 * LANES) == 0
            and depth % LANES == 0
            and hidden_here % (2 * n * ROWS) == 0
        )
        return fast_shards(n, *args) if fits else shards(*args)

    return run


def solution(mesh):
    placed = (
        P(("rep", "fs"), None),
        P(("rep", "fs"), None),
        P(("rep", "fs"), None),
        P("fs", "tp"),
        P("fs", "tp"),
        P("tp", "fs"),
        P("fs", "tp"),
        P("fs", "tp"),
        P("tp", "fs"),
    )
    return jax.shard_map(
        shards_for(mesh),
        mesh=mesh,
        in_specs=placed,
        out_specs=(
            P(("rep", "fs"), None),
            P(("rep", "fs"), None),
            P("fs", "tp"),
            P("fs", "tp"),
            P("tp", "fs"),
        ),
        check_vma=False,
    )
```

```python
import functools

import jax
import jax.numpy as jnp
from jax import lax
from jax.experimental import pallas as pl
from jax.experimental.pallas import tpu as pltpu
from jax.sharding import PartitionSpec as P

epsilon = 1e-06
MESH = pl.DeviceIdType.MESH
ANY = pl.BlockSpec(memory_space=pl.ANY)
LANES, ROWS = 128, 16


def contract_rows(left, right):
    return lax.dot_general(
        left, right, (((0,), (0,)), ((), ())), preferred_element_type=jnp.float32
    )


def contract_cols(left, right):
    return lax.dot_general(
        left, right, (((1,), (1,)), ((), ())), preferred_element_type=jnp.float32
    )


def greet(peers):
    barrier = pltpu.get_barrier_semaphore()
    for peer in peers:
        pl.semaphore_signal(barrier, inc=1, device_id=peer, device_id_type=MESH)
    pl.semaphore_wait(barrier, len(peers))


def push(src, dst, send_sem, recv_sem, peer):
    copy = pltpu.make_async_remote_copy(
        src_ref=src,
        dst_ref=dst,
        send_sem=send_sem,
        recv_sem=recv_sem,
        device_id=peer,
        device_id_type=MESH,
    )
    return copy


def block(index, size, unit):
    return pl.ds(pl.multiple_of(index * size, unit), size)


def call(body, outs, sems, collective, *args, scratch=()):
    return pl.pallas_call(
        body,
        out_shape=outs,
        in_specs=[ANY] * len(args),
        out_specs=jax.tree.map(lambda _: ANY, outs),
        scratch_shapes=[pltpu.SemaphoreType.DMA((n,)) for n in sems] + list(scratch),
        compiler_params=pltpu.CompilerParams(
            collective_id=collective, has_side_effects=True, vmem_limit_bytes=2**20
        ),
    )(*args)


def here():
    rep, fs, tp = lax.axis_index("rep"), lax.axis_index("fs"), lax.axis_index("tp")
    return rep, fs, tp, {"rep": 1 - rep}, {"tp": 1 - tp}


def gather_kernel(n, acts, weights, acts_all, weights_all, send, recv, wsend, wrecv):
    rep, fs, tp, twin, mate = here()
    line = n // 2
    z, y = fs // 2, lax.rem(fs, 2)
    side = {"fs": fs + 1 - 2 * y}
    rows, width = acts.shape[1], acts.shape[2]
    half = width // 2
    piece = weights_all.shape[1]
    part = piece // 2
    depth = weights.shape[2]
    mine = block(tp, half, LANES)
    greet([twin, mate] + [{"fs": lax.rem(fs + k, n)} for k in range(1, n)])

    def spot(origin):
        return acts_all.at[:, block(origin, rows, ROWS), mine]

    def other_spot(origin):
        return acts_all.at[:, block(origin, rows, ROWS), block(1 - tp, half, LANES)]

    right0, left0, side0, mate0 = 1, 1 + line, 1 + 2 * line, 1 + 3 * line
    own = acts.at[:, :, mine]
    up, down = {"fs": lax.rem(fs + 2, n)}, {"fs": lax.rem(fs + n - 2, n)}

    def go_up(s):
        src = own if s == 0 else spot(fs - 2 * s)
        return push(src, spot(fs - 2 * s), send.at[right0 + s], recv.at[right0 + s], up)

    def go_down(s):
        src = own if s == 0 else spot(fs + 2 * s)
        return push(src, spot(fs + 2 * s), send.at[left0 + s], recv.at[left0 + s], down)

    def go_side(s, sign):
        origin = fs + 2 * sign * s
        src = own if s == 0 else spot(origin)
        at = side0 + origin // 2
        return push(src, spot(origin), send.at[at], recv.at[at], side)

    def go_mate(origin):
        at = mate0 + origin
        return push(spot(origin), spot(origin), send.at[at], recv.at[at], mate)

    def weight(k):
        to = lax.rem(fs + k, n)
        src = weights.at[:, block(to * 2 + rep, part, ROWS), :]
        dst = weights_all.at[:, block(rep, part, ROWS), block(fs, depth, LANES)]
        return push(src, dst, wsend.at[k], wrecv.at[k], {"fs": to})

    def weight_on(k):
        origin = lax.rem(fs + n - k, n)
        ref = weights_all.at[:, block(rep, part, ROWS), block(origin, depth, LANES)]
        return push(ref, ref, wsend.at[n + k], wrecv.at[n + k], twin)

    def weight_from_twin(k):
        origin = lax.rem(fs + n - k, n)
        ref = weights_all.at[:, block(1 - rep, part, ROWS), block(origin, depth, LANES)]
        return push(ref, ref, wsend.at[n + k], wrecv.at[n + k], twin)

    own_weight = push(
        weights.at[:, block(fs, piece, ROWS), :],
        weights_all.at[:, :, block(fs, depth, LANES)],
        wsend.at[0],
        wrecv.at[0],
        twin,
    )
    own_mate = push(acts, acts_all.at[:, block(fs, rows, ROWS), :], send.at[0], recv.at[0], mate)

    has_up = lambda s: (z - s >= 0) & (z + 1 < line)
    has_down = lambda s: (z + s < line) & (z - 1 >= 0)
    from_below = lambda s: z - 1 - s >= 0
    from_above = lambda s: z + 1 + s < line

    pl.when(has_up(0))(lambda: go_up(0).start())
    pl.when(has_down(0))(lambda: go_down(0).start())
    go_side(0, 1).start()
    own_mate.start()
    own_weight.start()
    order = sorted(range(1, n), key=lambda k: -min(k, n - k))
    groups = [order[g :: line] for g in range(line)]

    for s in range(line - 1):
        for k in groups[s]:
            weight(k).start()

        def below():
            push(spot(fs - 2 * (s + 1)), spot(fs - 2 * (s + 1)), send.at[right0 + s], recv.at[right0 + s], up).wait_recv()
            if s + 1 < line - 1:
                pl.when(has_up(s + 1))(lambda: go_up(s + 1).start())
            go_side(s + 1, -1).start()
            go_mate(fs - 2 * (s + 1)).start()

        def above():
            push(spot(fs + 2 * (s + 1)), spot(fs + 2 * (s + 1)), send.at[left0 + s], recv.at[left0 + s], up).wait_recv()
            if s + 1 < line - 1:
                pl.when(has_down(s + 1))(lambda: go_down(s + 1).start())
            go_side(s + 1, 1).start()
            go_mate(fs + 2 * (s + 1)).start()

        pl.when(from_below(s))(below)
        pl.when(from_above(s))(above)
    for k in groups[line - 1]:
        weight(k).start()

    def side_in(place):
        origin = place * 2 + (1 - y)
        at = side0 + place
        push(spot(origin), spot(origin), send.at[at], recv.at[at], side).wait_recv()
        go_mate(origin).start()

    side_in(z)
    for k in order:
        origin = lax.rem(fs + n - k, n)
        ref = weights_all.at[:, block(rep, part, ROWS), block(origin, depth, LANES)]
        push(ref, ref, wsend.at[k], wrecv.at[k], twin).wait_recv()
        weight_on(k).start()
    for s in range(1, line):
        pl.when(z - s >= 0)(lambda: side_in(z - s))
        pl.when(z + s < line)(lambda: side_in(z + s))

    own_mate.wait()
    own_weight.wait()
    for k in range(1, n):
        weight_from_twin(k).wait_recv()
        weight_on(k).wait_send()
        weight(k).wait_send()
        origin = lax.rem(fs + k, n)
        at = mate0 + origin
        ref = other_spot(origin)
        push(ref, ref, send.at[at], recv.at[at], mate).wait()
    for s in range(line - 1):
        pl.when(has_up(s))(lambda: go_up(s).wait_send())
        pl.when(has_down(s))(lambda: go_down(s).wait_send())
    for place in range(line):
        ref = spot(place * 2 + y)
        push(ref, ref, send.at[side0 + place], recv.at[side0 + place], side).wait_send()


def add_rows(dst, left, right):
    strip = ROWS
    count = dst.shape[0] // strip

    @pl.loop(0, count)
    def _(i):
        at = pl.ds(pl.multiple_of(i * strip, strip), strip)
        total = left[at, :].astype(jnp.float32) + right[at, :].astype(jnp.float32)
        dst[at, :] = total.astype(dst.dtype)


def reduce_kernel(
    n,
    late,
    norm,
    gate_up,
    down,
    full,
    grads_all,
    p_in,
    p2,
    y_in,
    p3,
    z_in,
    g_in,
    g2,
    sums,
    send,
    recv,
    gsend,
    grecv,
    local,
):
    rep, fs, tp, twin, mate = here()
    line = n // 2
    z, y = fs // 2, lax.rem(fs, 2)
    side = {"fs": fs + 1 - 2 * y}
    half = sums.shape[2]
    rows = sums.shape[1]
    part = g2.shape[1]
    piece = 2 * part
    depth = grads_all.shape[2]
    mine, other = block(tp, half, LANES), block(1 - tp, half, LANES)
    greet([twin, mate] + [{"fs": lax.rem(fs + k, n)} for k in range(1, n)])
    order = sorted(range(1, line), key=lambda k: -min(k, line - k)) + [0]
    far = sorted(range(1, n), key=lambda k: -min(k, n - k))
    side0, line0, x0, last = 2 * line, 3 * line, 4 * line, 4 * line + 3

    def place(k):
        return lax.rem(z + k, line)

    def span(k):
        return block(place(k), 2 * rows, ROWS)

    def to_mate(i, k):
        src = (late, norm)[i].at[span(k), other]
        at = i * line + k
        return push(src, p_in.at[i, span(k), :], send.at[at], recv.at[at], mate)

    def to_side(k):
        src = p2.at[:, block(place(k) * 2 + 1 - y, rows, ROWS), :]
        at = side0 + k
        return push(src, y_in.at[:, place(k)], send.at[at], recv.at[at], side)

    def to_line(k):
        at = line0 + k
        return push(
            p3.at[k], z_in.at[k - 1], send.at[at], recv.at[at], {"fs": lax.rem(fs + 2 * k, n)}
        )

    def delta(a, who):
        if a < 2:
            return gate_up.at[block(2 * a + who, part, ROWS), :]
        return down.at[block(who, part, ROWS), :]

    def to_twin(a):
        return push(delta(a, 1 - rep), g_in.at[a], send.at[x0 + a], recv.at[x0 + a], twin)

    def slot(a, origin, who):
        return grads_all.at[a, block(origin * 2 + who, part, ROWS), :]

    def share(a, k):
        to = lax.rem(fs + k, n)
        src = g2.at[a, :, block(to, depth, LANES)]
        at = a * n + k
        return push(src, slot(a, fs, rep), gsend.at[at], grecv.at[at], {"fs": to})

    def share_in(a, k):
        ref = slot(a, lax.rem(fs + n - k, n), rep)
        at = a * n + k
        return push(ref, ref, gsend.at[at], grecv.at[at], twin)

    def share_on(a, k):
        ref = slot(a, lax.rem(fs + n - k, n), rep)
        at = (3 + a) * n + k
        return push(ref, ref, gsend.at[at], grecv.at[at], twin)

    def share_from_twin(a, k):
        ref = slot(a, lax.rem(fs + n - k, n), 1 - rep)
        at = (3 + a) * n + k
        return push(ref, ref, gsend.at[at], grecv.at[at], twin)

    def own(a):
        return g2.at[a, :, block(fs, depth, LANES)]

    def own_twin(a):
        at = (3 + a) * n
        return push(own(a), slot(a, fs, rep), gsend.at[at], grecv.at[at], twin)

    def own_put(a):
        return pltpu.make_async_copy(own(a), slot(a, fs, rep), local.at[a])

    def weight_step(a):
        to_twin(a).wait_recv()
        add_rows(g2.at[a], delta(a, rep), g_in.at[a])
        for k in far:
            share(a, k).start()
        own_twin(a).start()
        own_put(a).start()

    def forward(a):
        for k in far:
            share_in(a, k).wait_recv()
            share_on(a, k).start()

    for k in order:
        for i in range(2):
            to_mate(i, k).start()
    for a in range(3):
        to_twin(a).start()
    for k in order:
        for i in range(2):
            to_mate(i, k).wait_recv()
            src = (late, norm)[i].at[span(k), mine]
            add_rows(p2.at[i, span(k), :], src, p_in.at[i, span(k), :])
        to_side(k).start()
    weight_step(0)
    for step, k in enumerate(order):
        to_side(k).wait_recv()
        for i in range(2):
            src = p2.at[i, block(place(k) * 2 + y, rows, ROWS), :]
            add_rows(p3.at[k, i], src, y_in.at[i, place(k)])
        if k:
            to_line(k).start()
        if step < 2:
            weight_step(step + 1)
        if step >= 1:
            if step - 1 < 3:
                forward(step - 1)
    for a in range(max(len(order) - 1, 0), 3):
        forward(a)
    for k in order[:-1]:
        to_line(k).wait_recv()
    for i in range(2):

        @pl.loop(0, rows // ROWS)
        def _(j):
            at = pl.ds(pl.multiple_of(j * ROWS, ROWS), ROWS)
            total = p3[0, i, at, :].astype(jnp.float32)
            for k in range(1, line):
                total += z_in[k - 1, i, at, :].astype(jnp.float32)
            sums[i, at, :] = total.astype(sums.dtype)

    out = push(sums, full.at[:, :, mine], send.at[last], recv.at[last], mate)
    out.start()
    keep = pltpu.make_async_copy(sums, full.at[:, :, mine], local.at[3])
    keep.start()
    for a in range(3):
        own_put(a).wait()
        own_twin(a).wait_send()
        ref = slot(a, fs, 1 - rep)
        at = (3 + a) * n
        push(ref, ref, gsend.at[at], grecv.at[at], twin).wait_recv()
        to_twin(a).wait_send()
        for k in far:
            share(a, k).wait_send()
            share_on(a, k).wait_send()
            share_from_twin(a, k).wait_recv()
    for k in order:
        for i in range(2):
            to_mate(i, k).wait_send()
        to_side(k).wait_send()
        if k:
            to_line(k).wait_send()
    keep.wait()
    out.wait_send()
    push(sums, full.at[:, :, other], send.at[last], recv.at[last], mate).wait_recv()


def update_kernel(gate_sum, up_sum, down_sum, deltas, new_gate, new_up, new_down):
    new_gate[...] = gate_sum[...] + deltas[0].astype(jnp.float32).T
    new_up[...] = up_sum[...] + deltas[1].astype(jnp.float32).T
    new_down[...] = down_sum[...] + deltas[2].astype(jnp.float32)


def update(gate_sum, up_sum, down_sum, deltas):
    depth, hidden_here = gate_sum.shape
    step = next(b for b in (512, 256, 128) if hidden_here % b == 0)
    wide = pl.BlockSpec((depth, step), lambda i: (0, i))
    tall = pl.BlockSpec((step, depth), lambda i: (i, 0))
    size = depth * hidden_here
    return pl.pallas_call(
        update_kernel,
        grid=(hidden_here // step,),
        out_shape=[jax.ShapeDtypeStruct(v.shape, v.dtype) for v in (gate_sum, up_sum, down_sum)],
        in_specs=[wide, wide, tall, pl.BlockSpec((3, step, depth), lambda i: (0, i, 0))],
        out_specs=[wide, wide, tall],
        cost_estimate=pl.CostEstimate(flops=3 * size, bytes_accessed=30 * size, transcendentals=0),
    )(gate_sum, up_sum, down_sum, deltas)


def fast_shards(n, x_early, x_late, grad_out, w_gate, w_up, w_down, gate_sum, up_sum, down_sum):
    bf16, f32 = jnp.bfloat16, jnp.float32
    shape = jax.ShapeDtypeStruct
    rep, fs, tp = lax.axis_index("rep"), lax.axis_index("fs"), lax.axis_index("tp")
    line = n // 2
    y = lax.rem(fs, 2)
    rows, width = x_early.shape
    hidden_here, depth = w_down.shape
    piece = hidden_here // n
    half = width // 2
    early = x_early.astype(f32)
    late = x_late.astype(f32)
    scale_of = lambda v: lax.rsqrt(jnp.mean(v * v, axis=-1, keepdims=True) + epsilon)
    early_scale, late_scale = scale_of(early), scale_of(late)
    acts = jnp.stack(
        [(early * early_scale).astype(bf16), (late * late_scale).astype(bf16), grad_out]
    )
    weights = jnp.stack([w_gate.T, w_up.T, w_down])
    acts_all, weights_all = call(
        functools.partial(gather_kernel, n),
        [shape((3, n * rows, width), bf16), shape((3, piece, width), bf16)],
        (1 + 3 * line + n, 1 + 3 * line + n, 2 * n, 2 * n),
        0,
        acts,
        weights,
    )
    gate_t, up_t, down_t = weights_all[0], weights_all[1], weights_all[2]
    normed, cotangent = acts_all[0], acts_all[2]
    gate_up = weights_all[:2].reshape(2 * piece, width)
    def activations(rows_in):
        pre = contract_cols(rows_in, gate_up)
        gate_pre, up_pre = pre[:, :piece], pre[:, piece:]
        sig = jax.nn.sigmoid(gate_pre)
        return gate_pre, up_pre, sig, (gate_pre * sig * up_pre).astype(bf16)

    tokens = n * rows
    g, u, s, hidden = activations(normed)
    hidden_late = activations(acts_all[1])[3]
    late_part = jnp.dot(hidden_late, down_t, preferred_element_type=f32).astype(bf16)
    grad_hidden = 0.5 * contract_cols(cotangent, down_t)
    grad_gate_in = (grad_hidden * u * s * (1.0 + g * (1.0 - s))).astype(bf16)
    grad_up_in = (grad_hidden * g * s).astype(bf16)
    grads_in = jnp.concatenate([grad_gate_in, grad_up_in], axis=1)
    normed_part = jnp.dot(grads_in, gate_up, preferred_element_type=f32).astype(bf16)
    gate_up_delta = contract_rows(grads_in, normed).astype(bf16)
    down_delta = (0.5 * contract_rows(hidden, cotangent)).astype(bf16)
    part = piece // 2
    dma = pltpu.SemaphoreType.DMA
    vmem = pl.BlockSpec(memory_space=pltpu.VMEM)
    full, grads_all = pl.pallas_call(
        functools.partial(reduce_kernel, n),
        out_shape=[shape((2, rows, width), bf16), shape((3, hidden_here, depth), bf16)],
        in_specs=[vmem] * 4,
        out_specs=[ANY, ANY],
        scratch_shapes=[
            pltpu.VMEM((2, tokens, half), bf16),
            pltpu.VMEM((2, tokens, half), bf16),
            pltpu.VMEM((2, line, rows, half), bf16),
            pltpu.VMEM((line, 2, rows, half), bf16),
            pltpu.VMEM((line - 1, 2, rows, half), bf16),
            pltpu.VMEM((3, part, width), bf16),
            pltpu.VMEM((3, part, width), bf16),
            pltpu.VMEM((2, rows, half), bf16),
            dma((4 * line + 4,)),
            dma((4 * line + 4,)),
            dma((6 * n,)),
            dma((6 * n,)),
            dma((4,)),
        ],
        compiler_params=pltpu.CompilerParams(
            collective_id=1, has_side_effects=True, vmem_limit_bytes=48 * 2**20
        ),
    )(late_part, normed_part, gate_up_delta, down_delta)
    full = full.astype(f32)
    branch, grad_normed = full[0], full[1]
    out_late = (late + 0.5 * branch).astype(bf16)
    unit_rows = early * early_scale
    inner = jnp.mean(grad_normed * unit_rows, axis=-1, keepdims=True)
    grad_in = (
        grad_out.astype(f32) + early_scale * (grad_normed - unit_rows * inner)
    ).astype(bf16)
    return (out_late, grad_in, *update(gate_sum, up_sum, down_sum, grads_all))


def shards(x_early, x_late, grad_out, w_gate, w_up, w_down, gate_sum, up_sum, down_sum):
    gate_full, up_full, down_full = (
        lax.all_gather(w_gate, "fs", axis=0, tiled=True),
        lax.all_gather(w_up, "fs", axis=0, tiled=True),
        lax.all_gather(w_down, "fs", axis=1, tiled=True),
    )
    batch_rows = x_early.shape[0]
    stacked = jnp.concatenate([x_early, x_late], axis=0).astype(jnp.float32)
    row_scale = lax.rsqrt(jnp.mean(stacked * stacked, axis=-1, keepdims=True) + epsilon)
    normed = (stacked * row_scale).astype(jnp.bfloat16)
    gate_pre = jnp.dot(normed, gate_full, preferred_element_type=jnp.float32)
    up_pre = jnp.dot(normed, up_full, preferred_element_type=jnp.float32)
    gate_sig = jax.nn.sigmoid(gate_pre)
    hidden = (gate_pre * gate_sig * up_pre).astype(jnp.bfloat16)
    late_part = jnp.dot(hidden[batch_rows:], down_full, preferred_element_type=jnp.float32).astype(
        jnp.bfloat16
    )
    branch = lax.psum(late_part, "tp").astype(jnp.float32)
    out_late = (stacked[batch_rows:] + 0.5 * branch).astype(jnp.bfloat16)
    early_gate = gate_pre[:batch_rows]
    early_upper = up_pre[:batch_rows]
    early_sig = gate_sig[:batch_rows]
    early_hidden = hidden[:batch_rows]
    early_normed = normed[:batch_rows]
    early_scale = row_scale[:batch_rows]
    grad_hidden = 0.5 * contract_cols(grad_out, down_full)
    grad_gate_in = (
        grad_hidden * early_upper * early_sig * (1.0 + early_gate * (1.0 - early_sig))
    ).astype(jnp.bfloat16)
    grad_up_in = (grad_hidden * early_gate * early_sig).astype(jnp.bfloat16)
    normed_part = contract_cols(grad_gate_in, gate_full) + contract_cols(grad_up_in, up_full)
    grad_normed = lax.psum(normed_part.astype(jnp.bfloat16), "tp").astype(jnp.float32)
    unit_rows = stacked[:batch_rows] * early_scale
    inner = jnp.mean(grad_normed * unit_rows, axis=-1, keepdims=True)
    grad_in = (
        grad_out.astype(jnp.float32) + early_scale * (grad_normed - unit_rows * inner)
    ).astype(jnp.bfloat16)
    normed_cols, out_cols = (
        lax.all_to_all(early_normed, "fs", split_axis=1, concat_axis=0, tiled=True),
        lax.all_to_all(grad_out, "fs", split_axis=1, concat_axis=0, tiled=True),
    )
    gate_delta = contract_rows(normed_cols, lax.all_gather(grad_gate_in, "fs", axis=0, tiled=True))
    up_delta = contract_rows(normed_cols, lax.all_gather(grad_up_in, "fs", axis=0, tiled=True))
    down_half = contract_rows(lax.all_gather(early_hidden, "fs", axis=0, tiled=True), out_cols)
    down_delta = 0.5 * down_half
    gate_delta, up_delta, down_delta = (
        lax.psum(gate_delta.astype(jnp.bfloat16), "rep").astype(jnp.float32),
        lax.psum(up_delta.astype(jnp.bfloat16), "rep").astype(jnp.float32),
        lax.psum(down_delta.astype(jnp.bfloat16), "rep").astype(jnp.float32),
    )
    return (out_late, grad_in, gate_sum + gate_delta, up_sum + up_delta, down_sum + down_delta)


def shards_for(mesh):
    n, reps, cores = mesh.shape["fs"], mesh.shape["rep"], mesh.shape["tp"]

    def run(*args):
        rows, width = args[0].shape
        hidden_here, depth = args[5].shape
        fits = (
            reps == 2
            and cores == 2
            and n % 2 == 0
            and rows % ROWS == 0
            and width % (2 * LANES) == 0
            and depth % LANES == 0
            and hidden_here % (2 * n * ROWS) == 0
            and hidden_here % LANES == 0
        )
        return fast_shards(n, *args) if fits else shards(*args)

    return run


def solution(mesh):
    placed = (
        P(("rep", "fs"), None),
        P(("rep", "fs"), None),
        P(("rep", "fs"), None),
        P("fs", "tp"),
        P("fs", "tp"),
        P("tp", "fs"),
        P("fs", "tp"),
        P("fs", "tp"),
        P("tp", "fs"),
    )
    return jax.shard_map(
        shards_for(mesh),
        mesh=mesh,
        in_specs=placed,
        out_specs=(
            P(("rep", "fs"), None),
            P(("rep", "fs"), None),
            P("fs", "tp"),
            P("fs", "tp"),
            P("tp", "fs"),
        ),
        check_vma=False,
    )
```

```python
import functools

import jax
import jax.numpy as jnp
from jax import lax
from jax.experimental import pallas as pl
from jax.experimental.pallas import tpu as pltpu
from jax.sharding import PartitionSpec as P

epsilon = 1e-06
MESH = pl.DeviceIdType.MESH
ANY = pl.BlockSpec(memory_space=pl.ANY)
LANES, ROWS = 128, 16


def contract_rows(left, right):
    return lax.dot_general(
        left, right, (((0,), (0,)), ((), ())), preferred_element_type=jnp.float32
    )


def contract_cols(left, right):
    return lax.dot_general(
        left, right, (((1,), (1,)), ((), ())), preferred_element_type=jnp.float32
    )


def greet(peers):
    barrier = pltpu.get_barrier_semaphore()
    for peer in peers:
        pl.semaphore_signal(barrier, inc=1, device_id=peer, device_id_type=MESH)
    pl.semaphore_wait(barrier, len(peers))


def push(src, dst, send_sem, recv_sem, peer):
    copy = pltpu.make_async_remote_copy(
        src_ref=src,
        dst_ref=dst,
        send_sem=send_sem,
        recv_sem=recv_sem,
        device_id=peer,
        device_id_type=MESH,
    )
    return copy


def block(index, size, unit):
    return pl.ds(pl.multiple_of(index * size, unit), size)


def call(body, outs, sems, collective, *args, scratch=()):
    return pl.pallas_call(
        body,
        out_shape=outs,
        in_specs=[ANY] * len(args),
        out_specs=jax.tree.map(lambda _: ANY, outs),
        scratch_shapes=[pltpu.SemaphoreType.DMA((n,)) for n in sems] + list(scratch),
        compiler_params=pltpu.CompilerParams(
            collective_id=collective, has_side_effects=True, vmem_limit_bytes=2**20
        ),
    )(*args)


def here():
    rep, fs, tp = lax.axis_index("rep"), lax.axis_index("fs"), lax.axis_index("tp")
    return rep, fs, tp, {"rep": 1 - rep}, {"tp": 1 - tp}


def gather_kernel(n, acts, weights, acts_all, weights_all, send, recv, wsend, wrecv):
    rep, fs, tp, twin, mate = here()
    line = n // 2
    z, y = fs // 2, lax.rem(fs, 2)
    side = {"fs": fs + 1 - 2 * y}
    rows, width = acts.shape[1], acts.shape[2]
    half = width // 2
    piece = weights_all.shape[1]
    part = piece // 2
    depth = weights.shape[2]
    mine = block(tp, half, LANES)
    greet([twin, mate] + [{"fs": lax.rem(fs + k, n)} for k in range(1, n)])

    def spot(origin):
        return acts_all.at[:, block(origin, rows, ROWS), mine]

    def other_spot(origin):
        return acts_all.at[:, block(origin, rows, ROWS), block(1 - tp, half, LANES)]

    right0, left0, side0, mate0 = 1, 1 + line, 1 + 2 * line, 1 + 3 * line
    own = acts.at[:, :, mine]
    up, down = {"fs": lax.rem(fs + 2, n)}, {"fs": lax.rem(fs + n - 2, n)}

    def go_up(s):
        src = own if s == 0 else spot(fs - 2 * s)
        return push(src, spot(fs - 2 * s), send.at[right0 + s], recv.at[right0 + s], up)

    def go_down(s):
        src = own if s == 0 else spot(fs + 2 * s)
        return push(src, spot(fs + 2 * s), send.at[left0 + s], recv.at[left0 + s], down)

    def go_side(s, sign):
        origin = fs + 2 * sign * s
        src = own if s == 0 else spot(origin)
        at = side0 + origin // 2
        return push(src, spot(origin), send.at[at], recv.at[at], side)

    def go_mate(origin):
        at = mate0 + origin
        return push(spot(origin), spot(origin), send.at[at], recv.at[at], mate)

    def weight(k):
        to = lax.rem(fs + k, n)
        src = weights.at[:, block(to * 2 + rep, part, ROWS), :]
        dst = weights_all.at[:, block(rep, part, ROWS), block(fs, depth, LANES)]
        return push(src, dst, wsend.at[k], wrecv.at[k], {"fs": to})

    def weight_on(k):
        origin = lax.rem(fs + n - k, n)
        ref = weights_all.at[:, block(rep, part, ROWS), block(origin, depth, LANES)]
        return push(ref, ref, wsend.at[n + k], wrecv.at[n + k], twin)

    def weight_from_twin(k):
        origin = lax.rem(fs + n - k, n)
        ref = weights_all.at[:, block(1 - rep, part, ROWS), block(origin, depth, LANES)]
        return push(ref, ref, wsend.at[n + k], wrecv.at[n + k], twin)

    own_weight = push(
        weights.at[:, block(fs, piece, ROWS), :],
        weights_all.at[:, :, block(fs, depth, LANES)],
        wsend.at[0],
        wrecv.at[0],
        twin,
    )
    own_mate = push(acts, acts_all.at[:, block(fs, rows, ROWS), :], send.at[0], recv.at[0], mate)

    has_up = lambda s: (z - s >= 0) & (z + 1 < line)
    has_down = lambda s: (z + s < line) & (z - 1 >= 0)
    from_below = lambda s: z - 1 - s >= 0
    from_above = lambda s: z + 1 + s < line

    pl.when(has_up(0))(lambda: go_up(0).start())
    pl.when(has_down(0))(lambda: go_down(0).start())
    go_side(0, 1).start()
    own_mate.start()
    own_weight.start()
    order = sorted(range(1, n), key=lambda k: -min(k, n - k))
    groups = [order[g :: line] for g in range(line)]

    for s in range(line - 1):
        for k in groups[s]:
            weight(k).start()

        def below():
            push(spot(fs - 2 * (s + 1)), spot(fs - 2 * (s + 1)), send.at[right0 + s], recv.at[right0 + s], up).wait_recv()
            if s + 1 < line - 1:
                pl.when(has_up(s + 1))(lambda: go_up(s + 1).start())
            go_side(s + 1, -1).start()
            go_mate(fs - 2 * (s + 1)).start()

        def above():
            push(spot(fs + 2 * (s + 1)), spot(fs + 2 * (s + 1)), send.at[left0 + s], recv.at[left0 + s], up).wait_recv()
            if s + 1 < line - 1:
                pl.when(has_down(s + 1))(lambda: go_down(s + 1).start())
            go_side(s + 1, 1).start()
            go_mate(fs + 2 * (s + 1)).start()

        pl.when(from_below(s))(below)
        pl.when(from_above(s))(above)
    for k in groups[line - 1]:
        weight(k).start()

    def side_in(place):
        origin = place * 2 + (1 - y)
        at = side0 + place
        push(spot(origin), spot(origin), send.at[at], recv.at[at], side).wait_recv()
        go_mate(origin).start()

    side_in(z)
    for k in order:
        origin = lax.rem(fs + n - k, n)
        ref = weights_all.at[:, block(rep, part, ROWS), block(origin, depth, LANES)]
        push(ref, ref, wsend.at[k], wrecv.at[k], twin).wait_recv()
        weight_on(k).start()
    for s in range(1, line):
        pl.when(z - s >= 0)(lambda: side_in(z - s))
        pl.when(z + s < line)(lambda: side_in(z + s))

    own_mate.wait()
    own_weight.wait()
    for k in range(1, n):
        weight_from_twin(k).wait_recv()
        weight_on(k).wait_send()
        weight(k).wait_send()
        origin = lax.rem(fs + k, n)
        at = mate0 + origin
        ref = other_spot(origin)
        push(ref, ref, send.at[at], recv.at[at], mate).wait()
    for s in range(line - 1):
        pl.when(has_up(s))(lambda: go_up(s).wait_send())
        pl.when(has_down(s))(lambda: go_down(s).wait_send())
    for place in range(line):
        ref = spot(place * 2 + y)
        push(ref, ref, send.at[side0 + place], recv.at[side0 + place], side).wait_send()


def add_rows(dst, left, right):
    strip = ROWS
    count = dst.shape[0] // strip

    @pl.loop(0, count)
    def _(i):
        at = pl.ds(pl.multiple_of(i * strip, strip), strip)
        total = left[at, :].astype(jnp.float32) + right[at, :].astype(jnp.float32)
        dst[at, :] = total.astype(dst.dtype)


def reduce_kernel(
    n,
    late,
    norm,
    gate_up,
    down,
    full,
    grads_all,
    p_in,
    p2,
    y_in,
    p3,
    z_in,
    g_in,
    g2,
    sums,
    send,
    recv,
    gsend,
    grecv,
    local,
):
    rep, fs, tp, twin, mate = here()
    line = n // 2
    z, y = fs // 2, lax.rem(fs, 2)
    side = {"fs": fs + 1 - 2 * y}
    half = sums.shape[2]
    rows = sums.shape[1]
    part = g2.shape[1]
    piece = 2 * part
    depth = grads_all.shape[2]
    mine, other = block(tp, half, LANES), block(1 - tp, half, LANES)
    greet([twin, mate] + [{"fs": lax.rem(fs + k, n)} for k in range(1, n)])
    order = sorted(range(line), key=lambda d: (-abs(2 * d + 1 - line), -d))
    far = sorted(range(1, n), key=lambda k: -min(k, n - k))
    side0, line0, x0, last = 2 * line, 3 * line, 5 * line, 5 * line + 3
    above, below = {"fs": lax.rem(fs + 2, n)}, {"fs": lax.rem(fs + n - 2, n)}

    def span(k):
        return block(k, 2 * rows, ROWS)

    def to_mate(i, k):
        src = (late, norm)[i].at[span(k), other]
        at = i * line + k
        return push(src, p_in.at[i, span(k), :], send.at[at], recv.at[at], mate)

    def to_side(k):
        src = p2.at[:, block(k * 2 + 1 - y, rows, ROWS), :]
        at = side0 + k
        return push(src, y_in.at[:, k], send.at[at], recv.at[at], side)

    def go_up(d):
        at = line0 + d
        return push(p3.at[0, d], z_in.at[0, d], send.at[at], recv.at[at], above)

    def go_down(d):
        at = line0 + line + d
        return push(p3.at[1, d], z_in.at[1, d], send.at[at], recv.at[at], below)

    def chain(d):
        to_side(d).wait_recv()

        def make(way):
            for i in range(2):
                src = p2.at[i, block(d * 2 + y, rows, ROWS), :]
                add_rows(p3.at[way, d, i], src, y_in.at[i, d])

        def join(way, copy):
            copy.wait_recv()
            for i in range(2):
                add_rows(p3.at[way, d, i], p3.at[way, d, i], z_in.at[way, d, i])

        def rise():
            make(0)
            pl.when(z > 0)(lambda: join(0, go_up(d)))
            go_up(d).start()

        def fall():
            make(1)
            pl.when(z < line - 1)(lambda: join(1, go_down(d)))
            go_down(d).start()

        pl.when(z < d)(rise)
        pl.when(z > d)(fall)
        pl.when(z == d)(lambda: make(0))

    def delta(a, who):
        if a < 2:
            return gate_up.at[block(2 * a + who, part, ROWS), :]
        return down.at[block(who, part, ROWS), :]

    def to_twin(a):
        return push(delta(a, 1 - rep), g_in.at[a], send.at[x0 + a], recv.at[x0 + a], twin)

    def slot(a, origin, who):
        return grads_all.at[a, block(origin * 2 + who, part, ROWS), :]

    def share(a, k):
        to = lax.rem(fs + k, n)
        src = g2.at[a, :, block(to, depth, LANES)]
        at = a * n + k
        return push(src, slot(a, fs, rep), gsend.at[at], grecv.at[at], {"fs": to})

    def share_in(a, k):
        ref = slot(a, lax.rem(fs + n - k, n), rep)
        at = a * n + k
        return push(ref, ref, gsend.at[at], grecv.at[at], twin)

    def share_on(a, k):
        ref = slot(a, lax.rem(fs + n - k, n), rep)
        at = (3 + a) * n + k
        return push(ref, ref, gsend.at[at], grecv.at[at], twin)

    def share_from_twin(a, k):
        ref = slot(a, lax.rem(fs + n - k, n), 1 - rep)
        at = (3 + a) * n + k
        return push(ref, ref, gsend.at[at], grecv.at[at], twin)

    def own(a):
        return g2.at[a, :, block(fs, depth, LANES)]

    def own_twin(a):
        at = (3 + a) * n
        return push(own(a), slot(a, fs, rep), gsend.at[at], grecv.at[at], twin)

    def own_put(a):
        return pltpu.make_async_copy(own(a), slot(a, fs, rep), local.at[a])

    def weight_step(a):
        to_twin(a).wait_recv()
        add_rows(g2.at[a], delta(a, rep), g_in.at[a])
        for k in far:
            share(a, k).start()
        own_twin(a).start()
        own_put(a).start()

    def forward(a):
        for k in far:
            share_in(a, k).wait_recv()
            share_on(a, k).start()

    for k in order:
        for i in range(2):
            to_mate(i, k).start()
    for a in range(3):
        to_twin(a).start()
    for k in order:
        for i in range(2):
            to_mate(i, k).wait_recv()
            src = (late, norm)[i].at[span(k), mine]
            add_rows(p2.at[i, span(k), :], src, p_in.at[i, span(k), :])
        to_side(k).start()
    weight_step(0)
    for step, k in enumerate(order):
        chain(k)
        if step < 2:
            weight_step(step + 1)
        if step >= 1:
            if step - 1 < 3:
                forward(step - 1)
    for a in range(max(len(order) - 1, 0), 3):
        forward(a)
    for d in range(line):

        def finish():
            for way, there, copy in ((0, z > 0, go_up(d)), (1, z < line - 1, go_down(d))):

                def join():
                    copy.wait_recv()
                    for i in range(2):
                        add_rows(p3.at[0, d, i], p3.at[0, d, i], z_in.at[way, d, i])

                pl.when(there)(join)
            for i in range(2):

                @pl.loop(0, rows // ROWS)
                def _(j):
                    at = pl.ds(pl.multiple_of(j * ROWS, ROWS), ROWS)
                    sums[i, at, :] = p3[0, d, i, at, :]

        pl.when(z == d)(finish)
    out = push(sums, full.at[:, :, mine], send.at[last], recv.at[last], mate)
    out.start()
    keep = pltpu.make_async_copy(sums, full.at[:, :, mine], local.at[3])
    keep.start()
    for a in range(3):
        own_put(a).wait()
        own_twin(a).wait_send()
        ref = slot(a, fs, 1 - rep)
        at = (3 + a) * n
        push(ref, ref, gsend.at[at], grecv.at[at], twin).wait_recv()
        to_twin(a).wait_send()
        for k in far:
            share(a, k).wait_send()
            share_on(a, k).wait_send()
            share_from_twin(a, k).wait_recv()
    for k in order:
        for i in range(2):
            to_mate(i, k).wait_send()
        to_side(k).wait_send()
        pl.when(z < k)(lambda: go_up(k).wait_send())
        pl.when(z > k)(lambda: go_down(k).wait_send())
    keep.wait()
    out.wait_send()
    push(sums, full.at[:, :, other], send.at[last], recv.at[last], mate).wait_recv()


def update_kernel(gate_sum, up_sum, down_sum, deltas, new_gate, new_up, new_down):
    new_gate[...] = gate_sum[...] + deltas[0].astype(jnp.float32).T
    new_up[...] = up_sum[...] + deltas[1].astype(jnp.float32).T
    new_down[...] = down_sum[...] + deltas[2].astype(jnp.float32)


def update(gate_sum, up_sum, down_sum, deltas):
    depth, hidden_here = gate_sum.shape
    step = next(b for b in (512, 256, 128) if hidden_here % b == 0)
    wide = pl.BlockSpec((depth, step), lambda i: (0, i))
    tall = pl.BlockSpec((step, depth), lambda i: (i, 0))
    size = depth * hidden_here
    return pl.pallas_call(
        update_kernel,
        grid=(hidden_here // step,),
        out_shape=[jax.ShapeDtypeStruct(v.shape, v.dtype) for v in (gate_sum, up_sum, down_sum)],
        in_specs=[wide, wide, tall, pl.BlockSpec((3, step, depth), lambda i: (0, i, 0))],
        out_specs=[wide, wide, tall],
        cost_estimate=pl.CostEstimate(flops=3 * size, bytes_accessed=30 * size, transcendentals=0),
    )(gate_sum, up_sum, down_sum, deltas)


def fast_shards(n, x_early, x_late, grad_out, w_gate, w_up, w_down, gate_sum, up_sum, down_sum):
    bf16, f32 = jnp.bfloat16, jnp.float32
    shape = jax.ShapeDtypeStruct
    rep, fs, tp = lax.axis_index("rep"), lax.axis_index("fs"), lax.axis_index("tp")
    line = n // 2
    y = lax.rem(fs, 2)
    rows, width = x_early.shape
    hidden_here, depth = w_down.shape
    piece = hidden_here // n
    half = width // 2
    early = x_early.astype(f32)
    late = x_late.astype(f32)
    scale_of = lambda v: lax.rsqrt(jnp.mean(v * v, axis=-1, keepdims=True) + epsilon)
    early_scale, late_scale = scale_of(early), scale_of(late)
    acts = jnp.stack(
        [(early * early_scale).astype(bf16), (late * late_scale).astype(bf16), grad_out]
    )
    weights = jnp.stack([w_gate.T, w_up.T, w_down])
    acts_all, weights_all = call(
        functools.partial(gather_kernel, n),
        [shape((3, n * rows, width), bf16), shape((3, piece, width), bf16)],
        (1 + 3 * line + n, 1 + 3 * line + n, 2 * n, 2 * n),
        0,
        acts,
        weights,
    )
    gate_t, up_t, down_t = weights_all[0], weights_all[1], weights_all[2]
    normed, cotangent = acts_all[0], acts_all[2]
    gate_up = weights_all[:2].reshape(2 * piece, width)
    def activations(rows_in):
        pre = contract_cols(rows_in, gate_up)
        gate_pre, up_pre = pre[:, :piece], pre[:, piece:]
        sig = jax.nn.sigmoid(gate_pre)
        return gate_pre, up_pre, sig, (gate_pre * sig * up_pre).astype(bf16)

    tokens = n * rows
    g, u, s, hidden = activations(normed)
    hidden_late = activations(acts_all[1])[3]
    late_part = jnp.dot(hidden_late, down_t, preferred_element_type=f32).astype(bf16)
    grad_hidden = 0.5 * contract_cols(cotangent, down_t)
    grad_gate_in = (grad_hidden * u * s * (1.0 + g * (1.0 - s))).astype(bf16)
    grad_up_in = (grad_hidden * g * s).astype(bf16)
    grads_in = jnp.concatenate([grad_gate_in, grad_up_in], axis=1)
    normed_part = jnp.dot(grads_in, gate_up, preferred_element_type=f32).astype(bf16)
    gate_up_delta = contract_rows(grads_in, normed).astype(bf16)
    down_delta = (0.5 * contract_rows(hidden, cotangent)).astype(bf16)
    part = piece // 2
    dma = pltpu.SemaphoreType.DMA
    vmem = pl.BlockSpec(memory_space=pltpu.VMEM)
    full, grads_all = pl.pallas_call(
        functools.partial(reduce_kernel, n),
        out_shape=[shape((2, rows, width), bf16), shape((3, hidden_here, depth), bf16)],
        in_specs=[vmem] * 4,
        out_specs=[ANY, ANY],
        scratch_shapes=[
            pltpu.VMEM((2, tokens, half), bf16),
            pltpu.VMEM((2, tokens, half), bf16),
            pltpu.VMEM((2, line, rows, half), bf16),
            pltpu.VMEM((2, line, 2, rows, half), bf16),
            pltpu.VMEM((2, line, 2, rows, half), bf16),
            pltpu.VMEM((3, part, width), bf16),
            pltpu.VMEM((3, part, width), bf16),
            pltpu.VMEM((2, rows, half), bf16),
            dma((5 * line + 4,)),
            dma((5 * line + 4,)),
            dma((6 * n,)),
            dma((6 * n,)),
            dma((4,)),
        ],
        compiler_params=pltpu.CompilerParams(
            collective_id=1, has_side_effects=True, vmem_limit_bytes=48 * 2**20
        ),
    )(late_part, normed_part, gate_up_delta, down_delta)
    full = full.astype(f32)
    branch, grad_normed = full[0], full[1]
    out_late = (late + 0.5 * branch).astype(bf16)
    unit_rows = early * early_scale
    inner = jnp.mean(grad_normed * unit_rows, axis=-1, keepdims=True)
    grad_in = (
        grad_out.astype(f32) + early_scale * (grad_normed - unit_rows * inner)
    ).astype(bf16)
    return (out_late, grad_in, *update(gate_sum, up_sum, down_sum, grads_all))


def shards(x_early, x_late, grad_out, w_gate, w_up, w_down, gate_sum, up_sum, down_sum):
    gate_full, up_full, down_full = (
        lax.all_gather(w_gate, "fs", axis=0, tiled=True),
        lax.all_gather(w_up, "fs", axis=0, tiled=True),
        lax.all_gather(w_down, "fs", axis=1, tiled=True),
    )
    batch_rows = x_early.shape[0]
    stacked = jnp.concatenate([x_early, x_late], axis=0).astype(jnp.float32)
    row_scale = lax.rsqrt(jnp.mean(stacked * stacked, axis=-1, keepdims=True) + epsilon)
    normed = (stacked * row_scale).astype(jnp.bfloat16)
    gate_pre = jnp.dot(normed, gate_full, preferred_element_type=jnp.float32)
    up_pre = jnp.dot(normed, up_full, preferred_element_type=jnp.float32)
    gate_sig = jax.nn.sigmoid(gate_pre)
    hidden = (gate_pre * gate_sig * up_pre).astype(jnp.bfloat16)
    late_part = jnp.dot(hidden[batch_rows:], down_full, preferred_element_type=jnp.float32).astype(
        jnp.bfloat16
    )
    branch = lax.psum(late_part, "tp").astype(jnp.float32)
    out_late = (stacked[batch_rows:] + 0.5 * branch).astype(jnp.bfloat16)
    early_gate = gate_pre[:batch_rows]
    early_upper = up_pre[:batch_rows]
    early_sig = gate_sig[:batch_rows]
    early_hidden = hidden[:batch_rows]
    early_normed = normed[:batch_rows]
    early_scale = row_scale[:batch_rows]
    grad_hidden = 0.5 * contract_cols(grad_out, down_full)
    grad_gate_in = (
        grad_hidden * early_upper * early_sig * (1.0 + early_gate * (1.0 - early_sig))
    ).astype(jnp.bfloat16)
    grad_up_in = (grad_hidden * early_gate * early_sig).astype(jnp.bfloat16)
    normed_part = contract_cols(grad_gate_in, gate_full) + contract_cols(grad_up_in, up_full)
    grad_normed = lax.psum(normed_part.astype(jnp.bfloat16), "tp").astype(jnp.float32)
    unit_rows = stacked[:batch_rows] * early_scale
    inner = jnp.mean(grad_normed * unit_rows, axis=-1, keepdims=True)
    grad_in = (
        grad_out.astype(jnp.float32) + early_scale * (grad_normed - unit_rows * inner)
    ).astype(jnp.bfloat16)
    normed_cols, out_cols = (
        lax.all_to_all(early_normed, "fs", split_axis=1, concat_axis=0, tiled=True),
        lax.all_to_all(grad_out, "fs", split_axis=1, concat_axis=0, tiled=True),
    )
    gate_delta = contract_rows(normed_cols, lax.all_gather(grad_gate_in, "fs", axis=0, tiled=True))
    up_delta = contract_rows(normed_cols, lax.all_gather(grad_up_in, "fs", axis=0, tiled=True))
    down_half = contract_rows(lax.all_gather(early_hidden, "fs", axis=0, tiled=True), out_cols)
    down_delta = 0.5 * down_half
    gate_delta, up_delta, down_delta = (
        lax.psum(gate_delta.astype(jnp.bfloat16), "rep").astype(jnp.float32),
        lax.psum(up_delta.astype(jnp.bfloat16), "rep").astype(jnp.float32),
        lax.psum(down_delta.astype(jnp.bfloat16), "rep").astype(jnp.float32),
    )
    return (out_late, grad_in, gate_sum + gate_delta, up_sum + up_delta, down_sum + down_delta)


def shards_for(mesh):
    n, reps, cores = mesh.shape["fs"], mesh.shape["rep"], mesh.shape["tp"]

    def run(*args):
        rows, width = args[0].shape
        hidden_here, depth = args[5].shape
        fits = (
            reps == 2
            and cores == 2
            and n % 2 == 0
            and rows % ROWS == 0
            and width % (2 * LANES) == 0
            and depth % LANES == 0
            and hidden_here % (2 * n * ROWS) == 0
            and hidden_here % LANES == 0
        )
        return fast_shards(n, *args) if fits else shards(*args)

    return run


def solution(mesh):
    placed = (
        P(("rep", "fs"), None),
        P(("rep", "fs"), None),
        P(("rep", "fs"), None),
        P("fs", "tp"),
        P("fs", "tp"),
        P("tp", "fs"),
        P("fs", "tp"),
        P("fs", "tp"),
        P("tp", "fs"),
    )
    return jax.shard_map(
        shards_for(mesh),
        mesh=mesh,
        in_specs=placed,
        out_specs=(
            P(("rep", "fs"), None),
            P(("rep", "fs"), None),
            P("fs", "tp"),
            P("fs", "tp"),
            P("tp", "fs"),
        ),
        check_vma=False,
    )
```
